32 devices in a mesh: sp: 8 (over z, x), tp: 4 (over y, core).
Axes of the slice: x: 2, y: 2, z: 4, core: 2. Of those that a mesh axis runs over, the one named last changes fastest.
Arguments:
- latent: bfloat16 [4096, 2048], P(('sp', 'tp')), may hold values from -6 to 6
- context: bfloat16 [512, 2048], P('sp'), may hold values from -6 to 6
- conditioning: float32 [2048], P('sp'), may hold values from -6 to 6
- context_conditioning: float32 [2048], P('sp'), may hold values from -6 to 6
- shift_weight: bfloat16 [2048, 2048], P('sp', 'tp'), may hold values from -0.25 to 0.25
- scale_weight: bfloat16 [2048, 2048], P('sp', 'tp'), may hold values from -0.25 to 0.25
- gate_weight: bfloat16 [2048, 2048], P('sp', 'tp'), may hold values from -0.25 to 0.25
- norm_gain: float32 [2048], replicated, may hold values from 0.1 to 1.9
- query_weight: bfloat16 [2048, 2048], P(None, 'tp'), may hold values from -0.125 to 0.125
- key_weight: bfloat16 [2048, 1024], P(None, 'tp'), may hold values from -0.125 to 0.125
- value_weight: bfloat16 [2048, 1024], P(None, 'tp'), may hold values from -0.125 to 0.125
- query_gain: float32 [64], replicated, may hold values from 2 to 64, as said below
- key_gain: float32 [64], replicated, may hold values from 0.1 to 1.9
- context_lift: float32 [32], P('tp'), may hold values from 1.5 to 3
- output_weight: bfloat16 [2048, 2048], P('tp'), may hold values from -0.125 to 0.125
Outputs:
- mixed: bfloat16 [4096, 2048], P(('sp', 'tp'))
The draws below stay inside these ranges and needn't reach their ends.
Inputs may be any that keep to these rules, and one draw needn't show every extreme that they name: `query_gain`: one gain for each channel of a head.
All inputs are finite; a program needn't handle non-finite values.
Results may differ from the reference program's by a relative error of at most 0.018.
The reference program's roundings to bfloat16 on the way count: a program that leaves them out, or rounds other values in their place, can miss the bound.
Values may be sent and summed in bfloat16 or wider, within the bound.
A program may use at most 128 MiB of HBM per device.

```python
import math
import jax
import jax.numpy as jnp
from jax import lax

D = 2048
HEAD = 64
Q_HEADS = 32
KV_HEADS = 16
GRID = 64
CTX = 512
TOKENS = 4096


def draw_query_gain(key, part):
    base_key = jax.random.fold_in(key, 0)
    gains = jax.random.uniform(base_key, (HEAD,), jnp.float32, 2.0, 3.5)
    return gains


def block_scale(own_key, shape, cuts, smallest, largest):
    level = 1.0
    for dim, shards_of in cuts:
        steps = jax.random.uniform(jax.random.fold_in(jax.random.fold_in(own_key, 6), dim), (shards_of,), jnp.float32, smallest / len(cuts), largest / len(cuts))
        level = level * jnp.repeat(jnp.exp(steps), shape[dim] // shards_of).reshape((-1,) + (1,) * (len(shape) - 1 - dim))
    return level


def gaussian(key, shape, spread, reach, cuts=(), held_as=jnp.bfloat16):
    values = jax.random.normal(key, shape, jnp.float32) * spread
    if len(cuts) > 0:
        values = block_scale(key, shape, cuts, -0.22, 0.18) * values
    return jnp.clip(values, min=-reach, max=reach).astype(held_as)


def setup_inputs(seed: int = 0) -> dict:
    arg_keys = jax.random.split(jax.random.key(seed), 16)
    return {
        "latent": gaussian(arg_keys[0], (TOKENS, D), 1.0, 6.0, ((0, 32),)),
        "context": gaussian(arg_keys[1], (CTX, D), 1.0, 6.0, ((0, 8),)),
        "conditioning": gaussian(arg_keys[2], (D,), 1.0, 6.0, ((0, 8),), jnp.float32),
        "context_conditioning": gaussian(arg_keys[3], (D,), 1.0, 6.0, ((0, 8),), jnp.float32),
        "shift_weight": gaussian(arg_keys[4], (D, D), (D // 4) ** -0.5, 0.25, ((0, 8), (1, 4))),
        "scale_weight": gaussian(arg_keys[5], (D, D), (D // 4) ** -0.5, 0.25, ((0, 8), (1, 4))),
        "gate_weight": gaussian(arg_keys[6], (D, D), (D // 4) ** -0.5, 0.25, ((0, 8), (1, 4))),
        "norm_gain": jnp.clip(1.0 + 0.18 * jax.random.normal(arg_keys[7], (D,), jnp.float32), 0.1, 1.9),
        "query_weight": gaussian(arg_keys[8], (D, Q_HEADS * HEAD), D ** -0.5, 0.125, ((1, 4),)),
        "key_weight": gaussian(arg_keys[9], (D, KV_HEADS * HEAD), D ** -0.5, 0.125, ((1, 4),)),
        "value_weight": gaussian(arg_keys[10], (D, KV_HEADS * HEAD), D ** -0.5, 0.125, ((1, 4),)),
        "query_gain": draw_query_gain(jax.random.fold_in(arg_keys[15], 71), 0),
        "key_gain": jnp.clip(1.0 + 0.18 * jax.random.normal(arg_keys[12], (HEAD,), jnp.float32), 0.1, 1.9),
        "context_lift": jnp.clip(1.5 + 1.5 * jax.random.uniform(arg_keys[13], (Q_HEADS,), jnp.float32) ** block_scale(arg_keys[13], (Q_HEADS,), ((0, 4),), -0.2, 0.2), 1.5, 3.0),
        "output_weight": gaussian(arg_keys[14], (Q_HEADS * HEAD, D), (Q_HEADS * HEAD) ** -0.5, 0.125, ((0, 4),)),
    }


EPSILON = 1e-06
ROTARY_BASE = 10000.0

def normalize(values, gain):
    return values * lax.rsqrt(lax.optimization_barrier(jnp.mean(values * values, axis=-1, keepdims=True)) + EPSILON) * gain

def rotary_tables(offset, count):
    position = offset + jnp.arange(count, dtype=jnp.int32)
    grid_row = (position // GRID).astype(jnp.float32)
    grid_column = (position % GRID).astype(jnp.float32)
    quarter = HEAD // 4
    frequency = ROTARY_BASE ** (-jnp.arange(quarter, dtype=jnp.float32) / quarter)
    angles = jnp.concatenate([grid_row[:, None] * frequency, grid_column[:, None] * frequency], axis=1)
    return (jnp.repeat(jnp.cos(angles), 2, axis=1), jnp.repeat(jnp.sin(angles), 2, axis=1))

def rotate(values, cos_table, sin_table):
    pairs = values.reshape(values.shape[:-1] + (HEAD // 2, 2))
    turned = jnp.stack([-pairs[..., 1], pairs[..., 0]], axis=-1).reshape(values.shape)
    return values * cos_table[:, None, :] + turned * sin_table[:, None, :]

def attend_head(operands):
    head_queries, head_keys, head_values, head_context_keys, head_context_values, lift = operands
    tokens = head_queries.shape[0]
    group = head_queries.shape[1]
    block = math.gcd(tokens, 512)
    keys_wide = head_keys.astype(jnp.float32)
    values_wide = head_values.astype(jnp.float32)
    context_keys_wide = head_context_keys.astype(jnp.float32)
    context_values_wide = head_context_values.astype(jnp.float32)

    def one_block(query_block):
        query_wide = query_block.astype(jnp.float32)
        latent_scores = jnp.einsum('qgd,sd->gqs', query_wide, keys_wide) * HEAD ** (-0.5)
        context_scores = jnp.einsum('qgd,sd->gqs', query_wide, context_keys_wide) * HEAD ** (-0.5) + lift[:, None, None]
        top = jnp.maximum(lax.optimization_barrier(jnp.max(latent_scores, axis=-1)), lax.optimization_barrier(jnp.max(context_scores, axis=-1)))[..., None]
        latent_weights = jnp.exp(latent_scores - top)
        context_weights = jnp.exp(context_scores - top)
        total = lax.optimization_barrier(jnp.sum(latent_weights, axis=-1)) + lax.optimization_barrier(jnp.sum(context_weights, axis=-1))
        summed = jnp.einsum('gqs,sd->qgd', latent_weights.astype(jnp.bfloat16).astype(jnp.float32), values_wide)
        summed = summed + jnp.einsum('gqs,sd->qgd', context_weights.astype(jnp.bfloat16).astype(jnp.float32), context_values_wide)
        return (summed / jnp.transpose(total)[:, :, None]).astype(jnp.bfloat16)
    result = lax.map(one_block, head_queries.reshape(tokens // block, block, group, HEAD))
    return result.reshape(tokens, group, HEAD)

def reference(latent, context, conditioning, context_conditioning, shift_weight, scale_weight, gate_weight, norm_gain, query_weight, key_weight, value_weight, query_gain, key_gain, context_lift, output_weight):
    signals = jnp.stack([jax.nn.silu(conditioning), jax.nn.silu(context_conditioning)]).astype(jnp.bfloat16)
    shifts = jnp.dot(signals, shift_weight, preferred_element_type=jnp.float32)
    scales = jnp.dot(signals, scale_weight, preferred_element_type=jnp.float32)
    gate = jnp.dot(signals[0:1], gate_weight, preferred_element_type=jnp.float32)[0]
    hidden = (normalize(latent.astype(jnp.float32), norm_gain) * (1.0 + scales[0]) + shifts[0]).astype(jnp.bfloat16)
    context_hidden = (normalize(context.astype(jnp.float32), norm_gain) * (1.0 + scales[1]) + shifts[1]).astype(jnp.bfloat16)
    tokens = latent.shape[0]
    group = Q_HEADS // KV_HEADS
    cos_table, sin_table = rotary_tables(0, tokens)
    raw_queries = jnp.dot(hidden, query_weight, preferred_element_type=jnp.float32).reshape(tokens, Q_HEADS, HEAD)
    queries = rotate(normalize(raw_queries, query_gain), cos_table, sin_table).astype(jnp.bfloat16)
    raw_keys = jnp.dot(hidden, key_weight, preferred_element_type=jnp.float32).reshape(tokens, KV_HEADS, HEAD)
    keys = rotate(normalize(raw_keys, key_gain), cos_table, sin_table).astype(jnp.bfloat16)
    values = jnp.dot(hidden, value_weight, preferred_element_type=jnp.float32).astype(jnp.bfloat16).reshape(tokens, KV_HEADS, HEAD)
    raw_context_keys = jnp.dot(context_hidden, key_weight, preferred_element_type=jnp.float32).reshape(CTX, KV_HEADS, HEAD)
    context_keys = normalize(raw_context_keys, key_gain).astype(jnp.bfloat16)
    context_values = jnp.dot(context_hidden, value_weight, preferred_element_type=jnp.float32).astype(jnp.bfloat16).reshape(CTX, KV_HEADS, HEAD)
    operands = (jnp.transpose(queries.reshape(tokens, KV_HEADS, group, HEAD), (1, 0, 2, 3)), jnp.transpose(keys, (1, 0, 2)), jnp.transpose(values, (1, 0, 2)), jnp.transpose(context_keys, (1, 0, 2)), jnp.transpose(context_values, (1, 0, 2)), context_lift.reshape(KV_HEADS, group))
    attended = lax.map(attend_head, operands)
    attended = jnp.transpose(attended, (1, 0, 2, 3)).reshape(tokens, Q_HEADS * HEAD)
    projection = jnp.dot(attended, output_weight, preferred_element_type=jnp.float32)
    return (latent.astype(jnp.float32) + gate * projection).astype(jnp.bfloat16)
```

```python
import functools
import math

import jax
import jax.numpy as jnp
from jax import lax
from jax.experimental import pallas as pl
from jax.experimental.pallas import tpu as pltpu
from jax.sharding import PartitionSpec as P

HEAD = 64
GRID = 64
EPSILON = 1e-06
ROTARY_BASE = 10000.0
F32 = jnp.float32
BF16 = jnp.bfloat16
VMEM = pltpu.VMEM
TILE = 256
ONES = 16
NT_DIMS = (((1,), (1,)), ((), ()))


def dot(a, b):
    return jnp.dot(a, b, preferred_element_type=F32)


def dot_nt(a, b):
    return lax.dot_general(a, b, NT_DIMS, preferred_element_type=F32)


def remote(src, dst, send, recv, sp, tp):
    return pltpu.make_async_remote_copy(
        src_ref=src,
        dst_ref=dst,
        send_sem=send,
        recv_sem=recv,
        device_id=(sp, tp),
        device_id_type=pl.DeviceIdType.MESH,
    )


def loop(low, high, body):
    def step(i, _):
        body(i)
        return 0

    lax.fori_loop(low, high, step, 0)


def fused_kernel(
    n_sp, n_tp, groups, w_chunks, l_chunks,
    latent_h, context_h, cond, ctx_cond, shift_h, scale_h, gate_h, gain,
    wq_h, wk_h, wv_h, q_gain, k_gain, lift, wo_h,
    out,
    lat, ctxp, shift_w, scale_w, gate_w, wq, wk, wv, w_t, wo_all,
    part, total, recv1, recv2, mods, rows8, hid, cos_t, sin_t,
    qst, kst, vst, cst, qin, kin, vin, cin, kcx, vcx, qbd,
    sa, sb, m_ref, acc, ost, att_t, att,
    loads, s1, r1, s2, r2, sy, ry, sfw, rp,
    sq, rq, sk, rk, sv, rv, sc, rc,
    swy, rwy, swx, rwx, swp, rwp, swo, rwo, s_out, r_out,
):
    me = lax.axis_index("sp")
    t = lax.axis_index("tp")
    n_y = n_tp // 2
    y, c = t // 2, t % 2
    partner = y * 2 + 1 - c
    halves = n_sp // groups
    half, g = me // groups, me % groups
    rows, model = lat.shape[1], lat.shape[2]
    per_tile = TILE // rows
    n_tiles = rows * n_tp // TILE
    y_per = per_tile // 2
    own_block = t // per_tile
    c_rows = context_h.shape[0]
    width = total.shape[1]

    def block(k):
        return lax.rem(own_block + k, n_tiles)

    fetch = [
        pltpu.make_async_copy(src, dst, loads.at[i])
        for i, (src, dst) in enumerate(
            (
                (latent_h, lat.at[t]), (shift_h, shift_w), (scale_h, scale_w), (gate_h, gate_w),
                (wq_h, wq), (wk_h, wk), (wv_h, wv),
                (context_h, ctxp.at[pl.ds(0, c_rows)]), (wo_h, wo_all.at[t]),
            )
        )
    ]
    for copy in fetch:
        copy.start()
    barrier = pltpu.get_barrier_semaphore()

    def greet(sp, tp):
        pl.semaphore_signal(barrier, inc=1, device_id=(sp, tp), device_id_type=pl.DeviceIdType.MESH)

    loop(1, n_sp, lambda j: greet(lax.rem(me + j, n_sp), t))

    def greet_half(j):
        loop(1, n_tp, lambda i: greet(half * groups + j, lax.rem(t + i, n_tp)))

    loop(0, groups, greet_half)
    pl.semaphore_wait(barrier, n_sp - 1 + groups * (n_tp - 1))

    piece = rows // l_chunks
    fetch[0].wait()

    def y_copy(k, ch):
        other = lax.rem(y + k, n_y)
        part_of = lat.at[t, pl.ds(ch * piece, piece)]
        return remote(part_of, part_of, sy.at[k, ch], ry.at[t, ch], me, other * 2 + c)

    def y_start(ch):
        loop(1, n_y, lambda k: y_copy(k, ch).start())

    early = (l_chunks + 1) // 2
    for ch in range(early):
        y_start(ch)
    own_partner = remote(lat.at[t], lat.at[t], sfw.at[0, 0], rp.at[t, 0], me, partner)
    own_partner.start()

    shape8 = (8, cond.shape[1])
    row8 = lax.broadcasted_iota(jnp.int32, shape8, 0)
    a = jnp.broadcast_to(cond[...] / (1.0 + jnp.exp(-cond[...])), shape8)
    b = jnp.broadcast_to(ctx_cond[...] / (1.0 + jnp.exp(-ctx_cond[...])), shape8)
    first = jnp.where(row8 == 0, a, jnp.where(row8 == 1, b, 0.0)).astype(BF16)
    second = jnp.where(row8 == 2, a, jnp.where(row8 == 3, b, 0.0)).astype(BF16)
    third = jnp.where(row8 == 4, a, 0.0).astype(BF16)
    for copy in fetch[1:4]:
        copy.wait()
    mine = dot(first, shift_w[...]) + dot(second, scale_w[...]) + dot(third, gate_w[...])
    part[...] = mine
    recv1[me] = mine

    def mod_copy(j):
        return remote(part, recv1.at[me], s1.at[j], r1.at[me], lax.rem(me + j, n_sp), t)

    loop(1, n_sp, lambda j: mod_copy(j).start())

    for copy in fetch[4:7]:
        copy.wait()

    def turn_weights(i):
        span = pl.ds(pl.multiple_of(i * TILE, TILE), TILE)
        q_rows, k_rows, v_rows = (jnp.transpose(w[span, :]) for w in (wq, wk, wv))
        for j in range(groups):
            w_t[j, 0 : 2 * HEAD, span] = q_rows[2 * HEAD * j : 2 * HEAD * (j + 1), :]
            w_t[j, 2 * HEAD : 3 * HEAD, span] = k_rows[HEAD * j : HEAD * (j + 1), :]
            w_t[j, 3 * HEAD : 4 * HEAD, span] = v_rows[HEAD * j : HEAD * (j + 1), :]

    n_turns = model // TILE
    loop(0, n_turns // 2, turn_weights)

    def mod_wait(j):
        src = lax.rem(me + j, n_sp)
        pltpu.make_async_copy(recv1.at[src], recv1.at[src], r1.at[src]).wait()

    loop(1, n_sp, mod_wait)
    summed = lax.fori_loop(1, n_sp, lambda j, s: s + recv1[j], recv1[0])
    total[...] = summed
    recv2[t] = summed

    def tot_copy(j):
        return remote(total, recv2.at[t], s2.at[j], r2.at[t], me, lax.rem(t + j, n_tp))

    loop(1, n_tp, lambda j: tot_copy(j).start())
    for ch in range(early, l_chunks):
        y_start(ch)

    loop(n_turns // 2, n_turns, turn_weights)

    channel = lax.broadcasted_iota(jnp.int32, (HEAD, TILE), 0)
    lane = lax.broadcasted_iota(jnp.int32, (HEAD, TILE), 1)
    quarter = HEAD // 4
    power = ((channel // 2) % quarter).astype(F32)
    frequency = jnp.exp(power * (-math.log(ROTARY_BASE) / quarter))
    even = channel % 2 == 0

    def tables(i):
        position = (me * n_tiles + i) * TILE + lane
        place = jnp.where(channel < HEAD // 2, position // GRID, position % GRID)
        angle = place.astype(F32) * frequency
        cos_t[i] = jnp.cos(angle)
        sine = jnp.sin(angle)
        sin_t[i] = jnp.where(even, -sine, sine)

    loop(0, n_tiles, tables)

    def blank(i):
        qbd[i] = jnp.zeros(qbd.shape[1:], BF16)

    loop(0, qbd.shape[0], blank)

    def ones(ref, i):
        ref[i, HEAD:, :] = jnp.ones((ONES, TILE), BF16)

    loop(0, vin.shape[0], lambda i: ones(vin, i))
    loop(0, vcx.shape[0], lambda i: ones(vcx, i))

    def tot_wait(j):
        src = lax.rem(t + j, n_tp)
        pltpu.make_async_copy(recv2.at[src], recv2.at[src], r2.at[src]).wait()

    loop(1, n_tp, tot_wait)
    for j in range(n_tp):
        mods[:, j * width : (j + 1) * width] = recv2[j]
    for i, (shift_row, scale_row) in enumerate(((0, 2), (1, 3))):
        factor = gain[...] * (1.0 + mods[scale_row : scale_row + 1, :])
        rows8[2 * i] = jnp.broadcast_to(factor, (8, model))
        rows8[2 * i + 1] = jnp.broadcast_to(mods[shift_row : shift_row + 1, :], (8, model))

    step_rows = 32

    def hidden_of(x, which):
        x = x.astype(F32)
        inv = lax.rsqrt(jnp.mean(x * x, axis=-1, keepdims=True) + EPSILON)
        x = (x * inv).reshape(x.shape[0] // 8, 8, model)
        return (x * rows8[2 * which][None] + rows8[2 * which + 1][None]).reshape(-1, model)

    q_gains = jnp.broadcast_to(q_gain[...], (HEAD, TILE))
    k_gains = jnp.broadcast_to(k_gain[...], (HEAD, TILE))

    def norm(v, gains):
        mean = jnp.mean(v * v, axis=0, keepdims=True)
        return v * lax.rsqrt(mean + EPSILON) * gains

    def turn(v, cos_v, sin_v):
        v3 = v.reshape(HEAD // 8, 8, TILE)
        pairs = lax.broadcasted_iota(jnp.int32, v3.shape, 1) % 2 == 0
        swapped = jnp.where(pairs, pltpu.roll(v3, 7, 1), pltpu.roll(v3, 1, 1)).reshape(HEAD, TILE)
        return v * cos_v + swapped * sin_v

    def q_copy(bk, j, to):
        return remote(qst.at[bk, j], qin.at[g, bk], sq.at[bk, to], rq.at[g, bk], half * groups + j, t)

    def kv_copies(bk, n):
        j = lax.rem(g + n, groups)
        to = lax.rem(half + n // groups, halves) * groups + j
        slot = me * n_tiles + bk
        return (
            remote(kst.at[bk, j], kin.at[slot], sk.at[bk, n], rk.at[me, bk], to, t),
            remote(
                vst.at[bk, j], vin.at[slot, pl.ds(0, HEAD)], sv.at[bk, n], rv.at[me, bk], to, t
            ),
        )

    def project(bk):
        def hide(i):
            start = i * step_rows
            x = lat[bk * per_tile + start // rows, pl.ds(start % rows, step_rows), :]
            hid[pl.ds(pl.multiple_of(start, step_rows), step_rows), :] = hidden_of(x, 0).astype(BF16)

        loop(0, TILE // step_rows, hide)
        cos_v, sin_v = cos_t[bk], sin_t[bk]
        order = [lax.rem(g + n, groups) for n in list(range(1, groups)) + [0]]
        ahead = dot_nt(w_t[order[0]], hid[...])
        for place, j in enumerate(order):
            z = ahead
            if place + 1 < groups:
                ahead = dot_nt(w_t[order[place + 1]], hid[...])
            for i in range(2):
                q = turn(norm(z[HEAD * i : HEAD * (i + 1)], q_gains), cos_v, sin_v)
                qst[bk, j, i] = (q.astype(BF16).astype(F32) * HEAD ** (-0.5)).astype(BF16)
            k = turn(norm(z[2 * HEAD : 3 * HEAD], k_gains), cos_v, sin_v)
            k = jnp.concatenate([k[:, :128], k[:, 128:]], axis=0)
            kst[bk, j] = jnp.transpose(k).astype(BF16)
            vst[bk, j] = z[3 * HEAD :].astype(BF16)
            n = (place + 1) % groups
            if n:
                q_copy(bk, j, n).start()
                for copy in kv_copies(bk, n):
                    copy.start()
        qin[g, bk] = qst[bk, g]
        kin[me * n_tiles + bk] = kst[bk, g]
        vin[me * n_tiles + bk, 0:HEAD, :] = vst[bk, g]

        def cross(n):
            for copy in kv_copies(bk, n):
                copy.start()

        loop(groups, n_sp, cross)

    def y_near(other):
        return other * 2 + c, other * 2 + 1 - c

    def forward(other, ch):
        near, _ = y_near(other)
        part_of = lat.at[near, pl.ds(ch * piece, piece)]
        return remote(part_of, part_of, sfw.at[1 + other, ch], rp.at[near, ch], me, partner)

    def take(other):
        near, far = y_near(other)
        for ch in range(l_chunks):
            part_of = lat.at[near, pl.ds(ch * piece, piece)]
            pltpu.make_async_copy(part_of, part_of, ry.at[near, ch]).wait()
            forward(other, ch).start()
        for ch in range(l_chunks):
            part_of = lat.at[far, pl.ds(ch * piece, piece)]
            pltpu.make_async_copy(part_of, part_of, rp.at[far, ch]).wait()

    pltpu.make_async_copy(lat.at[partner], lat.at[partner], rp.at[partner, 0]).wait()
    if y_per > 1:
        loop(1, y_per, lambda o: take(own_block * y_per + lax.rem(y % y_per + o, y_per)))
    project(block(0))

    fetch[7].wait()
    c_lane = lax.broadcasted_iota(jnp.int32, (HEAD, 128), 1)

    def hide_context(i):
        span = pl.ds(pl.multiple_of(i * step_rows, step_rows), step_rows)
        row = i * step_rows + lax.broadcasted_iota(jnp.int32, (step_rows, model), 0)
        keep = row < c_rows
        h = hidden_of(jnp.where(keep, ctxp[span, :].astype(F32), 0.0), 1)
        hid[span, :] = jnp.where(keep, h, 0.0).astype(BF16)

    loop(0, 128 // step_rows, hide_context)
    for j in range(groups):
        z = dot_nt(w_t[j, 2 * HEAD :], hid[0:128, :])
        k = norm(z[:HEAD], k_gains[:, :128])
        cst[j] = jnp.where(c_lane < HEAD, k, pltpu.roll(z[HEAD:], HEAD, 1)).astype(BF16)

    def c_copy(n):
        to = lax.rem(half + n // groups, halves) * groups + lax.rem(g + n, groups)
        return remote(cst.at[lax.rem(g + n, groups)], cin.at[me], sc.at[n], rc.at[me], to, t)

    loop(1, n_sp, lambda n: c_copy(n).start())
    cin[me] = cst[g]

    fetch[8].wait()
    side = me % 2
    across = me + 1 - 2 * side

    def w_y(k, ch):
        other = lax.rem(y + k, n_y)
        ref = wo_all.at[t, side, ch]
        return remote(ref, ref, swy.at[k, ch], rwy.at[t, ch], me, other * 2 + c)

    def w_x(other, ch):
        near, _ = y_near(other)
        ref = wo_all.at[near, side, ch]
        return remote(ref, ref, swx.at[other, ch], rwx.at[near, ch], across, t)

    def w_p(other, ch, second):
        near, _ = y_near(other)
        ref = wo_all.at[near, 1 - side if second else side, ch]
        return remote(ref, ref, swp.at[other, ch, second], rwp.at[near, ch, second], me, partner)

    w_own = remote(wo_all.at[t], wo_all.at[t], swo, rwo, me, partner)

    def forward_y(ch):
        def one(k):
            other = lax.rem(y + n_y - k, n_y)
            near, _ = y_near(other)
            ref = wo_all.at[near, side, ch]
            pltpu.make_async_copy(ref, ref, rwy.at[near, ch]).wait()
            w_x(other, ch).start()
            w_p(other, ch, 0).start()

        loop(1, n_y, one)

    def forward_x(ch):
        def one(k):
            other = lax.rem(y + n_y - k, n_y)
            near, _ = y_near(other)
            ref = wo_all.at[near, 1 - side, ch]
            pltpu.make_async_copy(ref, ref, rwx.at[near, ch]).wait()
            w_p(other, ch, 1).start()

        loop(1, n_y, one)

    for ch in range(w_chunks):
        loop(1, n_y, lambda k, ch=ch: w_y(k, ch).start())
    w_own.start()

    for k in range(1, n_tiles):
        loop(0, y_per, lambda o, k=k: take(block(k) * y_per + o))
        project(block(k))

    def wait_kv(d, k, low):
        bk = block(k)

        def one(i):
            s = lax.rem(half + d, halves) * groups + lax.rem(g + i, groups)
            slot = s * n_tiles + bk
            pltpu.make_async_copy(kin.at[slot], kin.at[slot], rk.at[s, bk]).wait()
            ref = vin.at[slot, pl.ds(0, HEAD)]
            pltpu.make_async_copy(ref, ref, rv.at[s, bk]).wait()

        loop(low, groups, one)

    def wait_own(k):
        bk = block(k)

        def one(i):
            j = lax.rem(g + i, groups)
            pltpu.make_async_copy(qin.at[j, bk], qin.at[j, bk], rq.at[j, bk]).wait()

        loop(1, groups, one)
        wait_kv(0, k, 1)

        def spread(j):
            for i in range(2):
                q = qin[j, bk, i]
                slot = (j * n_tiles + bk) * 2 + i
                qbd[slot, 0:HEAD, 0:TILE] = q
                qbd[slot, HEAD:, TILE:] = q

        loop(0, groups, spread)

    def wait_cross(d, k):
        wait_kv(d, k, 0)

    def wait_context():
        def one(j):
            s = lax.rem(me + j, n_sp)
            pltpu.make_async_copy(cin.at[s], cin.at[s], rc.at[s]).wait()

        loop(1, n_sp, one)
        per = 128 // c_rows
        for u in range(kcx.shape[0]):
            keys, values = [], []
            for m in (2 * u, 2 * u + 1):
                k = v = jnp.zeros((HEAD, 128), F32)
                for i in range(per):
                    at = i * c_rows
                    both = cin[m * per + i].astype(F32)
                    keep = (c_lane >= at) & (c_lane < at + c_rows)
                    k = jnp.where(keep, pltpu.roll(both, at, 1) if at else both, k)
                    back = (at - HEAD) % 128
                    v = jnp.where(keep, pltpu.roll(both, back, 1) if back else both, v)
                keys.append(k)
                values.append(v)
            kcx[u] = jnp.transpose(jnp.concatenate(keys, axis=0)).astype(BF16)
            vcx[u, 0:HEAD, :] = jnp.concatenate(values, axis=1).astype(BF16)

    def slabs(d, k):
        base = lax.rem(half + d, halves) * groups
        slots = [(base + i) * n_tiles + block(k) for i in range(groups)]
        return [(kin, vin, slot, False) for slot in slots]

    context = [(kcx, vcx, u, True) for u in range(kcx.shape[0])]

    def out_copy(bk, j, p):
        return remote(
            ost.at[bk, j, p], att_t.at[t, g], s_out.at[bk, j, p], r_out.at[t, g],
            half * groups + j, bk * per_tile + p,
        )

    def sweep(k, blocks, start, final):
        bk = block(k)

        def slot_of(j, i):
            return (lax.rem(g + 1 + j, groups) * n_tiles + bk) * 2 + i

        def scores(j, i, dst):
            q = qbd[slot_of(j, i)]
            top = None
            for place, (keys, _, slot, lifted) in enumerate(blocks):
                s = dot(keys[slot], q)
                if lifted:
                    s = s + lift[g * 2 + i]
                dst[place] = s
                peak = jnp.max(s.reshape(s.shape[0] // 8, 8, s.shape[1]), axis=0)
                top = peak if top is None else jnp.maximum(top, peak)
            return top

        def soft(j, i, src, top):
            slot = slot_of(j, i)
            top = jnp.max(top, axis=0, keepdims=True)
            top = jnp.maximum(top[:, :TILE], top[:, TILE:])
            if not start:
                old = m_ref[slot, 0:1, :]
                top = jnp.maximum(old, top)
            wide = jnp.concatenate([top, top], axis=1)
            weights = []
            for place in range(len(blocks)):
                w = jnp.exp(src[place] - wide).astype(BF16)
                weights += [w[:, :TILE], w[:, TILE:]]
            values = jnp.concatenate([v[at] for _, v, at, _ in blocks], axis=1)
            o = dot(values, jnp.concatenate(weights, axis=0))
            if not start:
                o = acc[slot] * jnp.exp(old - top) + o
            if not final:
                acc[slot] = o
                m_ref[slot] = jnp.broadcast_to(top, (8, TILE))
                return
            o = (o[:HEAD] / o[HEAD : HEAD + 1]).astype(BF16)
            to = lax.rem(g + 1 + j, groups)
            for p in range(per_tile):
                ost[bk, to, p, i * HEAD : (i + 1) * HEAD, :] = o[:, p * rows : (p + 1) * rows]

        def pair(j, top):
            later = scores(j, 1, sb)
            soft(j, 0, sa, top)
            return later

        def body(j, top):
            later = pair(j, top)
            top = scores(j + 1, 0, sa)
            soft(j, 1, sb, later)
            if final:
                for p in range(per_tile):
                    out_copy(bk, lax.rem(g + 1 + j, groups), p).start()
            return top

        top = scores(0, 0, sa)
        top = lax.fori_loop(0, groups - 1, body, top)
        later = pair(groups - 1, top)
        soft(groups - 1, 1, sb, later)
        if final:
            for p in range(per_tile):
                if k:
                    out_copy(bk, g, p).start()
                else:

                    @pl.when(p != t % per_tile)
                    def _(p=p):
                        out_copy(bk, g, p).start()

            if k == 0:
                att_t[t, g] = ost[bk, g, t % per_tile]

    if n_tiles == 2 and halves == 2:
        wait_own(0)
        sweep(0, slabs(0, 0), True, False)
        wait_cross(1, 0)
        wait_context()
        sweep(0, slabs(1, 0) + context, False, False)
        wait_own(1)
        forward_y(0)
        sweep(1, slabs(0, 0) + slabs(0, 1) + context + slabs(1, 0), True, False)
        for ch in range(1, w_chunks - 1):
            forward_y(ch)
        forward_x(0)
        wait_cross(1, 1)
        sweep(1, slabs(1, 1), False, True)
        forward_y(w_chunks - 1)
        sweep(0, slabs(0, 1) + slabs(1, 1), False, True)
        for ch in range(1, w_chunks):
            forward_x(ch)
    else:
        for k in range(n_tiles):
            wait_own(k)
        wait_context()
        for k in range(n_tiles):
            own = [slab for i in range(n_tiles) for slab in slabs(0, i)]
            sweep(k, own + context, True, halves == 1)

        def further(d, final):
            for i in range(n_tiles):
                wait_cross(d, i)
            for k in range(n_tiles):
                sweep(k, [slab for i in range(n_tiles) for slab in slabs(d, i)], False, final)

        if halves > 1:
            loop(1, halves - 1, lambda d: further(d, False))
            further(halves - 1, True)
        for ch in range(w_chunks):
            forward_y(ch)
        for ch in range(w_chunks):
            forward_x(ch)

    ref = wo_all.at[partner]
    pltpu.make_async_copy(ref, ref, rwo).wait()

    def w_far(k):
        _, far = y_near(lax.rem(y + n_y - k, n_y))
        for ch in range(w_chunks):
            for second in range(2):
                ref = wo_all.at[far, 1 - side if second else side, ch]
                pltpu.make_async_copy(ref, ref, rwp.at[far, ch, second]).wait()

    loop(1, n_y, w_far)

    def out_wait(i):
        at = lax.rem(t * groups + g + i, n_tp * groups)
        ref = att_t.at[at // groups, at % groups]
        pltpu.make_async_copy(ref, ref, r_out.at[at // groups, at % groups]).wait()

    loop(1, n_tp * groups, out_wait)
    for i in range(n_tp):
        for j in range(groups):
            at = (i * groups + j) * 2 * HEAD
            att[:, at : at + 2 * HEAD] = jnp.transpose(att_t[i, j])
    n_out = 4
    wide = model // n_out
    for n in range(n_out):
        span = slice(n * wide, (n + 1) * wide)
        weight = wo_all[:, :, :, :, span].reshape(-1, wide)
        projection = dot(att[...], weight)
        out[:, span] = (lat[t, :, span].astype(F32) + mods[4:5, span] * projection).astype(BF16)

    own_partner.wait_send()
    w_own.wait_send()

    def drain_y(k):
        other = lax.rem(y + k, n_y)
        for ch in range(l_chunks):
            y_copy(k, ch).wait_send()
            forward(other, ch).wait_send()
        for ch in range(w_chunks):
            w_y(k, ch).wait_send()
            w_x(other, ch).wait_send()
            w_p(other, ch, 0).wait_send()
            w_p(other, ch, 1).wait_send()

    loop(1, n_y, drain_y)
    loop(1, n_sp, lambda j: mod_copy(j).wait_send())
    loop(1, n_tp, lambda j: tot_copy(j).wait_send())

    def drain_sp(n):
        c_copy(n).wait_send()
        for bk in range(n_tiles):
            for copy in kv_copies(bk, n):
                copy.wait_send()

    loop(1, n_sp, drain_sp)
    for bk in range(n_tiles):
        loop(1, groups, lambda n, bk=bk: q_copy(bk, lax.rem(g + n, groups), n).wait_send())

        def drain_out(j, bk=bk):
            for p in range(per_tile):

                @pl.when(jnp.logical_or(j != g, bk * per_tile + p != t))
                def _(p=p):
                    out_copy(bk, j, p).wait_send()

        loop(0, groups, drain_out)


def shards(
    n_sp, n_tp,
    latent, context, conditioning, context_conditioning, shift_weight, scale_weight, gate_weight,
    norm_gain, query_weight, key_weight, value_weight, query_gain, key_gain, context_lift, output_weight,
):
    k_heads = key_weight.shape[1] // HEAD
    q_heads = query_weight.shape[1] // HEAD
    rows, model = latent.shape
    c_rows = context.shape[0]
    o_rows = output_weight.shape[0]
    part_width = shift_weight.shape[1]
    assert q_heads == 2 * k_heads and n_sp % k_heads == 0 and n_sp % 2 == 0
    assert TILE % rows == 0 and rows * n_tp % TILE == 0 and 2 * c_rows <= 128
    groups = k_heads
    per_tile = TILE // rows
    n_tiles = rows * n_tp // TILE
    n_context = n_sp * c_rows // TILE
    w_chunks = 4 if o_rows >= 256 else 1
    l_chunks = 4 if rows >= 64 else 1
    most = groups * n_tiles * 2 + n_context
    n_q = groups * n_tiles * 2
    n_y = n_tp // 2
    vmem = pl.BlockSpec(memory_space=VMEM)
    dma = pltpu.SemaphoreType.DMA
    hbm = pl.BlockSpec(memory_space=pltpu.HBM)
    smem = pl.BlockSpec(memory_space=pltpu.SMEM)
    wo_shape = (2, w_chunks, o_rows // (2 * w_chunks), model)
    return pl.pallas_call(
        functools.partial(fused_kernel, n_sp, n_tp, groups, w_chunks, l_chunks),
        name="fused",
        out_shape=jax.ShapeDtypeStruct((rows, model), BF16),
        in_specs=[
            hbm, hbm, vmem, vmem, hbm, hbm, hbm, vmem, hbm, hbm, hbm, vmem, vmem, smem, hbm,
        ],
        out_specs=vmem,
        scratch_shapes=[
            VMEM((n_tp, rows, model), BF16), VMEM((128, model), BF16),
            VMEM(shift_weight.shape, BF16), VMEM(scale_weight.shape, BF16), VMEM(gate_weight.shape, BF16),
            VMEM(query_weight.shape, BF16), VMEM(key_weight.shape, BF16), VMEM(value_weight.shape, BF16),
            VMEM((groups, 4 * HEAD, model), BF16),
            VMEM((n_tp,) + wo_shape, BF16),
            VMEM((8, part_width), F32), VMEM((8, part_width), F32),
            VMEM((n_sp, 8, part_width), F32), VMEM((n_tp, 8, part_width), F32),
            VMEM((8, model), F32), VMEM((4, 8, model), F32),
            VMEM((TILE, model), BF16),
            VMEM((n_tiles, HEAD, TILE), F32), VMEM((n_tiles, HEAD, TILE), F32),
            VMEM((n_tiles, groups, 2, HEAD, TILE), BF16),
            VMEM((n_tiles, groups, 128, 128), BF16),
            VMEM((n_tiles, groups, HEAD, TILE), BF16),
            VMEM((groups, HEAD, 128), BF16),
            VMEM((groups, n_tiles, 2, HEAD, TILE), BF16),
            VMEM((n_sp * n_tiles, 128, 128), BF16),
            VMEM((n_sp * n_tiles, HEAD + ONES, TILE), BF16),
            VMEM((n_sp, HEAD, 128), BF16),
            VMEM((n_context, 128, 128), BF16),
            VMEM((n_context, HEAD + ONES, TILE), BF16),
            VMEM((n_q, 128, 2 * TILE), BF16),
            VMEM((most, 128, 2 * TILE), F32), VMEM((most, 128, 2 * TILE), F32),
            VMEM((n_q, 8, TILE), F32), VMEM((n_q, HEAD + ONES, TILE), F32),
            VMEM((n_tiles, groups, per_tile, 2 * HEAD, rows), BF16),
            VMEM((n_tp, groups, 2 * HEAD, rows), BF16),
            VMEM((rows, n_tp * groups * 2 * HEAD), BF16),
            dma((9,)), dma((n_sp,)), dma((n_sp,)), dma((n_tp,)), dma((n_tp,)),
            dma((n_y, l_chunks)), dma((n_tp, l_chunks)), dma((1 + n_y, l_chunks)), dma((n_tp, l_chunks)),
            dma((n_tiles, groups)), dma((groups, n_tiles)),
            dma((n_tiles, n_sp)), dma((n_sp, n_tiles)), dma((n_tiles, n_sp)), dma((n_sp, n_tiles)),
            dma((n_sp,)), dma((n_sp,)),
            dma((n_y, w_chunks)), dma((n_tp, w_chunks)), dma((n_y, w_chunks)), dma((n_tp, w_chunks)),
            dma((n_y, w_chunks, 2)), dma((n_tp, w_chunks, 2)), dma, dma,
            dma((n_tiles, groups, per_tile)), dma((n_tp, groups)),
        ],
        compiler_params=pltpu.CompilerParams(
            collective_id=0, has_side_effects=True, vmem_limit_bytes=60 * 1024 * 1024
        ),
    )(
        latent, context, conditioning[None], context_conditioning[None],
        shift_weight, scale_weight, gate_weight, norm_gain[None],
        query_weight, key_weight, value_weight,
        query_gain[:, None], key_gain[:, None], context_lift, output_weight.reshape(wo_shape),
    )


def solution(mesh):
    n_sp, n_tp = mesh.shape["sp"], mesh.shape["tp"]
    in_specs = (
        P(("sp", "tp"), None), P("sp", None), P("sp"), P("sp"),
        P("sp", "tp"), P("sp", "tp"), P("sp", "tp"), P(),
        P(None, "tp"), P(None, "tp"), P(None, "tp"), P(), P(), P("tp"), P("tp", None),
    )
    body = functools.partial(shards, n_sp, n_tp)
    return jax.shard_map(body, mesh=mesh, in_specs=in_specs, out_specs=P(("sp", "tp"), None), check_vma=False)
```

```python
import functools
import math

import jax
import jax.numpy as jnp
from jax import lax
from jax.experimental import pallas as pl
from jax.experimental.pallas import tpu as pltpu
from jax.sharding import PartitionSpec as P

HEAD = 64
GRID = 64
EPSILON = 1e-06
ROTARY_BASE = 10000.0
F32 = jnp.float32
BF16 = jnp.bfloat16
VMEM = pltpu.VMEM
TILE = 256
ONES = 16
NT_DIMS = (((1,), (1,)), ((), ()))


def dot(a, b):
    return jnp.dot(a, b, preferred_element_type=F32)


def dot_nt(a, b):
    return lax.dot_general(a, b, NT_DIMS, preferred_element_type=F32)


def remote(src, dst, send, recv, sp, tp):
    return pltpu.make_async_remote_copy(
        src_ref=src,
        dst_ref=dst,
        send_sem=send,
        recv_sem=recv,
        device_id=(sp, tp),
        device_id_type=pl.DeviceIdType.MESH,
    )


def loop(low, high, body):
    def step(i, _):
        body(i)
        return 0

    lax.fori_loop(low, high, step, 0)


def few(low, high, body):
    if high - low > 16:
        loop(low, high, body)
    else:
        for i in range(low, high):
            body(i)


def fused_kernel(
    n_sp, n_tp, groups, n_x, n_z, plain, l_chunks,
    latent_h, context_h, cond, ctx_cond, shift_h, scale_h, gate_h, gain,
    wq_h, wk_h, wv_h, q_gain, k_gain, lift, wo_h,
    out,
    lat, ctxp, shift_w, scale_w, gate_w, wq, wk, wv, w_t, wo_all,
    part, total, recv1, recv2, mods, rows8, hid, cos_t, sin_t,
    qst, kst, vst, cst, qin, kin, vin, cin, kcx, vcx, qbd,
    sa, sb, m_ref, acc, ost, att_t, att,
    loads, s1, r1, s2, r2, sy, ry, sfw, rp,
    sq, rq, sk, rk, sv, rv, sc, rc,
    swy, rwy, swx, rwx, swp, rwp, swo, rwo, s_out, r_out,
):
    me = lax.axis_index("sp")
    t = lax.axis_index("tp")
    n_y = n_tp // 2
    y, c = t // 2, t % 2
    partner = y * 2 + 1 - c
    halves = n_sp // groups
    half, g = me // groups, me % groups
    rows, model = lat.shape[1], lat.shape[2]
    per_tile = TILE // rows
    n_tiles = rows * n_tp // TILE
    y_per = per_tile // 2
    own_block = t // per_tile
    c_rows = context_h.shape[0]
    width = total.shape[1]

    def block(k):
        return lax.rem(own_block + k, n_tiles)

    fetch = [
        pltpu.make_async_copy(src, dst, loads.at[i])
        for i, (src, dst) in enumerate(
            (
                (latent_h, lat.at[t]), (shift_h, shift_w), (scale_h, scale_w), (gate_h, gate_w),
                (wq_h, wq), (wk_h, wk), (wv_h, wv),
                (context_h, ctxp.at[pl.ds(0, c_rows)]), (wo_h, wo_all.at[t]),
            )
        )
    ]
    for copy in fetch:
        copy.start()
    barrier = pltpu.get_barrier_semaphore()

    def greet(sp, tp):
        pl.semaphore_signal(barrier, inc=1, device_id=(sp, tp), device_id_type=pl.DeviceIdType.MESH)

    def greet_half(i):
        to = lax.rem(t + 1 + i // groups, n_tp)
        greet(half * groups + lax.rem(g + i, groups), to)

    few(1, n_sp, lambda j: greet(lax.rem(me + j, n_sp), t))
    few(0, groups * (n_tp - 1), greet_half)
    pl.semaphore_wait(barrier, n_sp - 1 + groups * (n_tp - 1))

    piece = rows // l_chunks
    fetch[0].wait()

    def y_copy(k, ch):
        other = lax.rem(y + k, n_y)
        part_of = lat.at[t, pl.ds(ch * piece, piece)]
        return remote(part_of, part_of, sy.at[k, ch], ry.at[t, ch], me, other * 2 + c)

    def y_start(ch):
        loop(1, n_y, lambda k: y_copy(k, ch).start())

    early = (l_chunks + 1) * 2 // 5
    early = max(early, 1)
    for ch in range(early):
        y_start(ch)
    own_partner = remote(lat.at[t], lat.at[t], sfw.at[0, 0], rp.at[t, 0], me, partner)
    own_partner.start()

    shape8 = (8, cond.shape[1])
    row8 = lax.broadcasted_iota(jnp.int32, shape8, 0)
    a = jnp.broadcast_to(cond[...] / (1.0 + jnp.exp(-cond[...])), shape8)
    b = jnp.broadcast_to(ctx_cond[...] / (1.0 + jnp.exp(-ctx_cond[...])), shape8)
    first = jnp.where(row8 == 0, a, jnp.where(row8 == 1, b, 0.0)).astype(BF16)
    second = jnp.where(row8 == 2, a, jnp.where(row8 == 3, b, 0.0)).astype(BF16)
    third = jnp.where(row8 == 4, a, 0.0).astype(BF16)
    for copy in fetch[1:4]:
        copy.wait()
    mine = dot(first, shift_w[...]) + dot(second, scale_w[...]) + dot(third, gate_w[...])
    part[...] = mine
    recv1[me] = mine

    def mod_copy(j):
        return remote(part, recv1.at[me], s1.at[j], r1.at[me], lax.rem(me + j, n_sp), t)

    loop(1, n_sp, lambda j: mod_copy(j).start())

    for copy in fetch[4:7]:
        copy.wait()

    def turn_weights(i):
        span = pl.ds(pl.multiple_of(i * TILE, TILE), TILE)
        q_rows, k_rows, v_rows = (jnp.transpose(w[span, :]) for w in (wq, wk, wv))
        for j in range(groups):
            w_t[j, 0 : 2 * HEAD, span] = q_rows[2 * HEAD * j : 2 * HEAD * (j + 1), :]
            w_t[j, 2 * HEAD : 3 * HEAD, span] = k_rows[HEAD * j : HEAD * (j + 1), :]
            w_t[j, 3 * HEAD : 4 * HEAD, span] = v_rows[HEAD * j : HEAD * (j + 1), :]

    n_turns = model // TILE
    loop(0, n_turns // 2, turn_weights)

    def mod_wait(j):
        src = lax.rem(me + j, n_sp)
        pltpu.make_async_copy(recv1.at[src], recv1.at[src], r1.at[src]).wait()

    loop(1, n_sp, mod_wait)
    summed = lax.fori_loop(1, n_sp, lambda j, s: s + recv1[j], recv1[0])
    total[...] = summed
    recv2[t] = summed

    def tot_copy(j):
        return remote(total, recv2.at[t], s2.at[j], r2.at[t], me, lax.rem(t + j, n_tp))

    loop(1, n_tp, lambda j: tot_copy(j).start())
    for ch in range(early, l_chunks):
        y_start(ch)

    loop(n_turns // 2, n_turns, turn_weights)

    channel = lax.broadcasted_iota(jnp.int32, (HEAD, TILE), 0)
    lane = lax.broadcasted_iota(jnp.int32, (HEAD, TILE), 1)
    quarter = HEAD // 4
    power = ((channel // 2) % quarter).astype(F32)
    frequency = jnp.exp(power * (-math.log(ROTARY_BASE) / quarter))
    even = channel % 2 == 0

    def tables(i):
        position = (me * n_tiles + i) * TILE + lane
        place = jnp.where(channel < HEAD // 2, position // GRID, position % GRID)
        angle = place.astype(F32) * frequency
        cos_t[i] = jnp.cos(angle)
        sine = jnp.sin(angle)
        sin_t[i] = jnp.where(even, -sine, sine)

    loop(0, n_tiles, tables)

    def blank(i):
        qbd[i] = jnp.zeros(qbd.shape[1:], BF16)

    loop(0, qbd.shape[0], blank)

    def ones(ref, i):
        ref[i, HEAD:, :] = jnp.ones((ONES, TILE), BF16)

    loop(0, vin.shape[0], lambda i: ones(vin, i))
    loop(0, vcx.shape[0], lambda i: ones(vcx, i))

    def tot_wait(j):
        src = lax.rem(t + j, n_tp)
        pltpu.make_async_copy(recv2.at[src], recv2.at[src], r2.at[src]).wait()

    loop(1, n_tp, tot_wait)
    for j in range(n_tp):
        mods[:, j * width : (j + 1) * width] = recv2[j]
    for i, (shift_row, scale_row) in enumerate(((0, 2), (1, 3))):
        factor = gain[...] * (1.0 + mods[scale_row : scale_row + 1, :])
        rows8[2 * i] = jnp.broadcast_to(factor, (8, model))
        rows8[2 * i + 1] = jnp.broadcast_to(mods[shift_row : shift_row + 1, :], (8, model))

    step_rows = 32

    def hidden_of(x, which):
        x = x.astype(F32)
        inv = lax.rsqrt(jnp.mean(x * x, axis=-1, keepdims=True) + EPSILON)
        x = (x * inv).reshape(x.shape[0] // 8, 8, model)
        return (x * rows8[2 * which][None] + rows8[2 * which + 1][None]).reshape(-1, model)

    def column(row):
        turned = jnp.transpose(jnp.broadcast_to(row[...], (128, HEAD)))
        return jnp.concatenate([turned] * (TILE // 128), axis=1)

    q_gains, k_gains = column(q_gain), column(k_gain)

    def norm(v, gains):
        mean = jnp.mean(v * v, axis=0, keepdims=True)
        return v * lax.rsqrt(mean + EPSILON) * gains

    def turn(v, cos_v, sin_v):
        v3 = v.reshape(HEAD // 8, 8, TILE)
        pairs = lax.broadcasted_iota(jnp.int32, v3.shape, 1) % 2 == 0
        swapped = jnp.where(pairs, pltpu.roll(v3, 7, 1), pltpu.roll(v3, 1, 1)).reshape(HEAD, TILE)
        return v * cos_v + swapped * sin_v

    def q_copy(bk, j, to):
        return remote(qst.at[bk, j], qin.at[g, bk], sq.at[bk, to], rq.at[g, bk], half * groups + j, t)

    def kv_copies(bk, n):
        j = lax.rem(g + n, groups)
        to = lax.rem(half + n // groups, halves) * groups + j
        slot = me * n_tiles + bk
        return (
            remote(kst.at[bk, j], kin.at[slot], sk.at[bk, n], rk.at[me, bk], to, t),
            remote(
                vst.at[bk, j], vin.at[slot, pl.ds(0, HEAD)], sv.at[bk, n], rv.at[me, bk], to, t
            ),
        )

    def hide(owner):
        base = lax.rem(owner, per_tile) * rows

        def one(i):
            x = lat[owner, pl.ds(i * step_rows, step_rows), :]
            start = pl.multiple_of(base + i * step_rows, step_rows)
            hid[pl.ds(start, step_rows), :] = hidden_of(x, 0).astype(BF16)

        loop(0, rows // step_rows, one)

    border = (half == 0) == (g >= groups // 2) if halves == 2 else g >= 0

    def project(bk):
        cos_v, sin_v = cos_t[bk], sin_t[bk]
        order = [lax.rem(g + n, groups) for n in list(range(1, groups)) + [0]]
        ahead = dot_nt(w_t[order[0]], hid[...])
        for place, j in enumerate(order):
            z = ahead
            if place + 1 < groups:
                ahead = dot_nt(w_t[order[place + 1]], hid[...])
            for i in range(2):
                q = turn(norm(z[HEAD * i : HEAD * (i + 1)], q_gains), cos_v, sin_v)
                qst[bk, j, i] = (q.astype(BF16).astype(F32) * HEAD ** (-0.5)).astype(BF16)
            k = turn(norm(z[2 * HEAD : 3 * HEAD], k_gains), cos_v, sin_v)
            k = jnp.concatenate([k[:, :128], k[:, 128:]], axis=0)
            kst[bk, j] = jnp.transpose(k).astype(BF16)
            vst[bk, j] = z[3 * HEAD :].astype(BF16)
            n = (place + 1) % groups
            if n:
                q_copy(bk, j, n).start()
                for copy in kv_copies(bk, n):
                    copy.start()

            @pl.when(border)
            def _(n=n):
                for d in range(1, halves):
                    for copy in kv_copies(bk, d * groups + n):
                        copy.start()

        qin[g, bk] = qst[bk, g]
        kin[me * n_tiles + bk] = kst[bk, g]
        vin[me * n_tiles + bk, 0:HEAD, :] = vst[bk, g]

    def cross(bk):
        def one(n):
            for copy in kv_copies(bk, n):
                copy.start()

        loop(groups, n_sp, one)

    def y_near(other):
        return other * 2 + c, other * 2 + 1 - c

    def forward(other, ch):
        near, _ = y_near(other)
        part_of = lat.at[near, pl.ds(ch * piece, piece)]
        return remote(part_of, part_of, sfw.at[1 + other, ch], rp.at[near, ch], me, partner)

    def take(other):
        near, far = y_near(other)
        for ch in range(l_chunks):
            part_of = lat.at[near, pl.ds(ch * piece, piece)]
            pltpu.make_async_copy(part_of, part_of, ry.at[near, ch]).wait()
            forward(other, ch).start()
        hide(near)
        for ch in range(l_chunks):
            part_of = lat.at[far, pl.ds(ch * piece, piece)]
            pltpu.make_async_copy(part_of, part_of, rp.at[far, ch]).wait()
        hide(far)

    hide(t)
    pltpu.make_async_copy(lat.at[partner], lat.at[partner], rp.at[partner, 0]).wait()
    hide(partner)
    if y_per > 1:
        loop(1, y_per, lambda o: take(own_block * y_per + lax.rem(y % y_per + o, y_per)))
    project(block(0))
    fetch[7].wait()
    c_lane = lax.broadcasted_iota(jnp.int32, (HEAD, 128), 1)

    def hide_context(i):
        span = pl.ds(pl.multiple_of(i * step_rows, step_rows), step_rows)
        row = i * step_rows + lax.broadcasted_iota(jnp.int32, (step_rows, model), 0)
        keep = row < c_rows
        h = hidden_of(jnp.where(keep, ctxp[span, :].astype(F32), 0.0), 1)
        hid[span, :] = jnp.where(keep, h, 0.0).astype(BF16)

    loop(0, 128 // step_rows, hide_context)
    for j in range(groups):
        z = dot_nt(w_t[j, 2 * HEAD :], hid[0:128, :])
        k = norm(z[:HEAD], k_gains[:, :128])
        cst[j] = jnp.where(c_lane < HEAD, k, pltpu.roll(z[HEAD:], HEAD, 1)).astype(BF16)

    def c_copy(n):
        to = lax.rem(half + n // groups, halves) * groups + lax.rem(g + n, groups)
        return remote(cst.at[lax.rem(g + n, groups)], cin.at[me], sc.at[n], rc.at[me], to, t)

    loop(1, n_sp, lambda n: c_copy(n).start())
    cin[me] = cst[g]

    fetch[8].wait()
    shared = n_x + n_z
    side_x, side_z = me % 2, g // (groups // 2 if groups > 1 else 1) % 2
    across_x = me + 1 - 2 * side_x
    across_z = half * groups + lax.rem(g + groups // 2, groups)

    def w_ref(owner, at):
        return wo_all.at[owner, at]

    def w_at(ch, mine=True):
        if ch < n_x:
            return (side_x if mine else 1 - side_x) * n_x + ch
        if ch < shared:
            return 2 * n_x + (side_z if mine else 1 - side_z) * n_z + ch - n_x
        return shared + ch

    def w_y(k, ch):
        other = lax.rem(y + k, n_y)
        ref = w_ref(t, w_at(ch))
        return remote(ref, ref, swy.at[k, ch], rwy.at[t, ch], me, other * 2 + c)

    def w_x(other, ch):
        near, _ = y_near(other)
        ref = w_ref(near, w_at(ch))
        return remote(ref, ref, swx.at[other, ch], rwx.at[near, ch], across_x if ch < n_x else across_z, t)

    def w_p(other, ch, mine=True):
        near, _ = y_near(other)
        at = w_at(ch, mine)
        ref = w_ref(near, at)
        return remote(ref, ref, swp.at[other, at], rwp.at[near, at], me, partner)

    w_own = remote(wo_all.at[t], wo_all.at[t], swo, rwo, me, partner)

    def over_y(body):
        loop(1, n_y, lambda k: body(lax.rem(y + n_y - k, n_y)))

    def forward_y(ch, to_x=True):
        def one(other):
            near, _ = y_near(other)
            ref = w_ref(near, w_at(ch))
            pltpu.make_async_copy(ref, ref, rwy.at[near, ch]).wait()
            if to_x:
                w_x(other, ch).start()
            w_p(other, ch).start()

        over_y(one)

    def forward_x(ch):
        def one(other):
            near, _ = y_near(other)
            ref = w_ref(near, w_at(ch, False))
            pltpu.make_async_copy(ref, ref, rwx.at[near, ch]).wait()
            w_p(other, ch, False).start()

        over_y(one)

    def forward_plain(ch):
        forward_y(shared + ch, False)

    for ch in range(shared + plain):
        loop(1, n_y, lambda k, ch=ch: w_y(k, ch).start())

    for k in range(1, n_tiles):
        loop(0, y_per, lambda o, k=k: take(block(k) * y_per + o))
        project(block(k))
    w_own.start()

    @pl.when(jnp.logical_not(border))
    def _():
        for k in range(n_tiles):
            cross(block(k))

    def wait_kv(d, k, low, high, first):
        bk = block(k)

        def one(i):
            s = lax.rem(half + d, halves) * groups + lax.rem(first + i, groups)
            slot = s * n_tiles + bk
            pltpu.make_async_copy(kin.at[slot], kin.at[slot], rk.at[s, bk]).wait()
            ref = vin.at[slot, pl.ds(0, HEAD)]
            pltpu.make_async_copy(ref, ref, rv.at[s, bk]).wait()

        loop(low, high, one)

    def wait_own(k):
        bk = block(k)

        def one(i):
            j = lax.rem(g + i, groups)
            pltpu.make_async_copy(qin.at[j, bk], qin.at[j, bk], rq.at[j, bk]).wait()

        loop(1, groups, one)
        wait_kv(0, k, 1, groups, g)

        def spread(j):
            for i in range(2):
                q = qin[j, bk, i]
                slot = (j * n_tiles + bk) * 2 + i
                qbd[slot, 0:HEAD, 0:TILE] = q
                qbd[slot, HEAD:, TILE:] = q

        loop(0, groups, spread)

    def wait_cross(d, k):
        wait_kv(d, k, 0, groups, 0)

    def wait_context():
        def one(j):
            s = lax.rem(me + j, n_sp)
            pltpu.make_async_copy(cin.at[s], cin.at[s], rc.at[s]).wait()

        loop(1, n_sp, one)
        per = 128 // c_rows
        for u in range(kcx.shape[0]):
            keys, values = [], []
            for m in (2 * u, 2 * u + 1):
                k = v = jnp.zeros((HEAD, 128), F32)
                for i in range(per):
                    at = i * c_rows
                    both = cin[m * per + i].astype(F32)
                    keep = (c_lane >= at) & (c_lane < at + c_rows)
                    k = jnp.where(keep, pltpu.roll(both, at, 1) if at else both, k)
                    back = (at - HEAD) % 128
                    v = jnp.where(keep, pltpu.roll(both, back, 1) if back else both, v)
                keys.append(k)
                values.append(v)
            kcx[u] = jnp.transpose(jnp.concatenate(keys, axis=0)).astype(BF16)
            vcx[u, 0:HEAD, :] = jnp.concatenate(values, axis=1).astype(BF16)

    def slabs(d, k, first=0, count=groups):
        base = lax.rem(half + d, halves) * groups
        slots = [(base + first + i) * n_tiles + block(k) for i in range(count)]
        return [(kin, vin, slot, False) for slot in slots]

    context = [(kcx, vcx, u, True) for u in range(kcx.shape[0])]

    def out_copy(bk, j, p):
        return remote(
            ost.at[bk, j, p], att_t.at[t, g], s_out.at[bk, j, p], r_out.at[t, g],
            half * groups + j, bk * per_tile + p,
        )

    def hooks(actions):
        def at(j):
            for when, action in actions.items():
                pl.when(j == when)(action)

        return at

    def sweep(k, blocks, start, final, hook=None):
        bk = block(k)

        def slot_of(j, i):
            return (lax.rem(g + 1 + j, groups) * n_tiles + bk) * 2 + i

        def scores(j, i, dst):
            q = qbd[slot_of(j, i)]
            top = None
            for place, (keys, _, slot, lifted) in enumerate(blocks):
                s = dot(keys[slot], q)
                if lifted:
                    s = s + lift[g * 2 + i]
                dst[place] = s
                peak = jnp.max(s.reshape(s.shape[0] // 8, 8, s.shape[1]), axis=0)
                top = peak if top is None else jnp.maximum(top, peak)
            return top

        def soft(j, i, src, top):
            slot = slot_of(j, i)
            top = jnp.max(top, axis=0, keepdims=True)
            top = jnp.maximum(top[:, :TILE], top[:, TILE:])
            if not start:
                old = m_ref[slot, 0:1, :]
                top = jnp.maximum(old, top)
            wide = jnp.concatenate([top, top], axis=1)
            weights = []
            for place in range(len(blocks)):
                w = jnp.exp(src[place] - wide).astype(BF16)
                weights += [w[:, :TILE], w[:, TILE:]]
            values = jnp.concatenate([v[at] for _, v, at, _ in blocks], axis=1)
            o = dot(values, jnp.concatenate(weights, axis=0))
            if not start:
                o = acc[slot] * jnp.exp(old - top) + o
            if not final:
                acc[slot] = o
                m_ref[slot] = jnp.broadcast_to(top, (8, TILE))
                return
            o = (o[:HEAD] / o[HEAD : HEAD + 1]).astype(BF16)
            to = lax.rem(g + 1 + j, groups)
            for p in range(per_tile):
                ost[bk, to, p, i * HEAD : (i + 1) * HEAD, :] = o[:, p * rows : (p + 1) * rows]

        def pair(j, top):
            later = scores(j, 1, sb)
            soft(j, 0, sa, top)
            return later

        def body(j, top):
            later = pair(j, top)
            top = scores(j + 1, 0, sa)
            soft(j, 1, sb, later)
            if hook is not None:
                hook(j)
            if final:
                for p in range(per_tile):
                    out_copy(bk, lax.rem(g + 1 + j, groups), p).start()
            return top

        top = scores(0, 0, sa)
        top = lax.fori_loop(0, groups - 1, body, top)
        later = pair(groups - 1, top)
        soft(groups - 1, 1, sb, later)
        if final:
            for p in range(per_tile):
                if k:
                    out_copy(bk, g, p).start()
                else:

                    @pl.when(p != t % per_tile)
                    def _(p=p):
                        out_copy(bk, g, p).start()

            if k == 0:
                att_t[t, g] = ost[bk, g, t % per_tile]

    if n_tiles == 2 and halves == 2 and groups == 4 and shared == 7:
        near_g = jnp.where(half == 0, 0, groups // 2)
        far_g = groups // 2 - near_g
        near, close = slabs(1, 0, near_g, 2), slabs(1, 1, near_g, 2)
        far0, far1 = slabs(1, 0, far_g, 2), slabs(1, 1, far_g, 2)
        wait_own(0)
        forward_y(0)
        sweep(0, slabs(0, 0), True, False)
        forward_y(1)
        wait_kv(1, 0, 0, 2, near_g)
        wait_context()
        sweep(0, near + context, False, False)
        forward_y(2)
        wait_own(1)
        own = slabs(0, 0) + slabs(0, 1) + context + near
        sweep(1, own, True, False, hooks({1: lambda: forward_y(3)}))
        forward_y(4)
        forward_y(5)
        forward_x(0)
        sweep(0, slabs(0, 1), False, False)
        forward_y(6)
        forward_x(1)
        wait_kv(1, 1, 0, 2, near_g)
        wait_kv(1, 0, 0, 2, far_g)
        wait_kv(1, 1, 0, 2, far_g)
        far = close + far0 + far1
        forward_plain(0)
        forward_x(2)
        sweep(1, far, False, True)
        forward_plain(1)
        forward_x(3)
        sweep(0, far, False, True)
        forward_x(4)
        forward_x(5)
        forward_x(6)
    else:
        for k in range(n_tiles):
            wait_own(k)
        wait_context()
        for k in range(n_tiles):
            own = [slab for i in range(n_tiles) for slab in slabs(0, i)]
            sweep(k, own + context, True, halves == 1)

        def further(d, final):
            for i in range(n_tiles):
                wait_cross(d, i)
            for k in range(n_tiles):
                sweep(k, [slab for i in range(n_tiles) for slab in slabs(d, i)], False, final)

        if halves > 1:
            loop(1, halves - 1, lambda d: further(d, False))
            further(halves - 1, True)
        for ch in range(shared):
            forward_y(ch)
        for ch in range(plain):
            forward_plain(ch)
        for ch in range(shared):
            forward_x(ch)

    ref = wo_all.at[partner]
    pltpu.make_async_copy(ref, ref, rwo).wait()

    def w_far(k):
        _, far = y_near(lax.rem(y + n_y - k, n_y))
        for at in range(2 * shared + plain):
            ref = w_ref(far, at)
            pltpu.make_async_copy(ref, ref, rwp.at[far, at]).wait()

    loop(1, n_y, w_far)

    def out_wait(i):
        at = lax.rem(t * groups + g + i, n_tp * groups)
        ref = att_t.at[at // groups, at % groups]
        pltpu.make_async_copy(ref, ref, r_out.at[at // groups, at % groups]).wait()

    loop(1, n_tp * groups, out_wait)
    for i in range(n_tp):
        for j in range(groups):
            at = (i * groups + j) * 2 * HEAD
            att[:, at : at + 2 * HEAD] = jnp.transpose(att_t[i, j])
    n_out = 4
    wide = model // n_out
    for n in range(n_out):
        span = slice(n * wide, (n + 1) * wide)
        weight = wo_all[:, :, :, span].reshape(-1, wide)
        projection = dot(att[...], weight)
        out[:, span] = (lat[t, :, span].astype(F32) + mods[4:5, span] * projection).astype(BF16)

    own_partner.wait_send()
    w_own.wait_send()

    def drain_y(k):
        other = lax.rem(y + k, n_y)
        for ch in range(l_chunks):
            y_copy(k, ch).wait_send()
            forward(other, ch).wait_send()
        for ch in range(shared + plain):
            w_y(k, ch).wait_send()
            w_p(other, ch).wait_send()
        for ch in range(shared):
            w_x(other, ch).wait_send()
            w_p(other, ch, False).wait_send()

    loop(1, n_y, drain_y)
    loop(1, n_sp, lambda j: mod_copy(j).wait_send())
    loop(1, n_tp, lambda j: tot_copy(j).wait_send())

    def drain_sp(n):
        c_copy(n).wait_send()
        for bk in range(n_tiles):
            for copy in kv_copies(bk, n):
                copy.wait_send()

    loop(1, n_sp, drain_sp)
    for bk in range(n_tiles):
        loop(1, groups, lambda n, bk=bk: q_copy(bk, lax.rem(g + n, groups), n).wait_send())

        def drain_out(j, bk=bk):
            for p in range(per_tile):

                @pl.when(jnp.logical_or(j != g, bk * per_tile + p != t))
                def _(p=p):
                    out_copy(bk, j, p).wait_send()

        loop(0, groups, drain_out)


def shards(
    n_sp, n_tp,
    latent, context, conditioning, context_conditioning, shift_weight, scale_weight, gate_weight,
    norm_gain, query_weight, key_weight, value_weight, query_gain, key_gain, context_lift, output_weight,
):
    k_heads = key_weight.shape[1] // HEAD
    q_heads = query_weight.shape[1] // HEAD
    rows, model = latent.shape
    c_rows = context.shape[0]
    o_rows = output_weight.shape[0]
    part_width = shift_weight.shape[1]
    assert q_heads == 2 * k_heads and n_sp % k_heads == 0 and n_sp % 2 == 0
    assert TILE % rows == 0 and rows * n_tp % TILE == 0 and 2 * c_rows <= 128
    groups = k_heads
    per_tile = TILE // rows
    n_tiles = rows * n_tp // TILE
    n_context = n_sp * c_rows // TILE
    n_x, n_z, plain = (5, 2, 2) if o_rows >= 256 and groups == 4 else (1, 0, 0)
    shared = n_x + n_z
    pieces = 2 * shared + plain
    l_chunks = 8 if rows >= 128 else 1
    most = groups * n_tiles * 2 + n_context
    n_q = groups * n_tiles * 2
    n_y = n_tp // 2
    vmem = pl.BlockSpec(memory_space=VMEM)
    dma = pltpu.SemaphoreType.DMA
    hbm = pl.BlockSpec(memory_space=pltpu.HBM)
    smem = pl.BlockSpec(memory_space=pltpu.SMEM)
    wo_shape = (pieces, o_rows // pieces, model)
    return pl.pallas_call(
        functools.partial(fused_kernel, n_sp, n_tp, groups, n_x, n_z, plain, l_chunks),
        name="fused",
        out_shape=jax.ShapeDtypeStruct((rows, model), BF16),
        in_specs=[
            hbm, hbm, vmem, vmem, hbm, hbm, hbm, vmem, hbm, hbm, hbm, vmem, vmem, smem, hbm,
        ],
        out_specs=vmem,
        scratch_shapes=[
            VMEM((n_tp, rows, model), BF16), VMEM((128, model), BF16),
            VMEM(shift_weight.shape, BF16), VMEM(scale_weight.shape, BF16), VMEM(gate_weight.shape, BF16),
            VMEM(query_weight.shape, BF16), VMEM(key_weight.shape, BF16), VMEM(value_weight.shape, BF16),
            VMEM((groups, 4 * HEAD, model), BF16),
            VMEM((n_tp,) + wo_shape, BF16),
            VMEM((8, part_width), F32), VMEM((8, part_width), F32),
            VMEM((n_sp, 8, part_width), F32), VMEM((n_tp, 8, part_width), F32),
            VMEM((8, model), F32), VMEM((4, 8, model), F32),
            VMEM((TILE, model), BF16),
            VMEM((n_tiles, HEAD, TILE), F32), VMEM((n_tiles, HEAD, TILE), F32),
            VMEM((n_tiles, groups, 2, HEAD, TILE), BF16),
            VMEM((n_tiles, groups, 128, 128), BF16),
            VMEM((n_tiles, groups, HEAD, TILE), BF16),
            VMEM((groups, HEAD, 128), BF16),
            VMEM((groups, n_tiles, 2, HEAD, TILE), BF16),
            VMEM((n_sp * n_tiles, 128, 128), BF16),
            VMEM((n_sp * n_tiles, HEAD + ONES, TILE), BF16),
            VMEM((n_sp, HEAD, 128), BF16),
            VMEM((n_context, 128, 128), BF16),
            VMEM((n_context, HEAD + ONES, TILE), BF16),
            VMEM((n_q, 128, 2 * TILE), BF16),
            VMEM((most, 128, 2 * TILE), F32), VMEM((most, 128, 2 * TILE), F32),
            VMEM((n_q, 8, TILE), F32), VMEM((n_q, HEAD + ONES, TILE), F32),
            VMEM((n_tiles, groups, per_tile, 2 * HEAD, rows), BF16),
            VMEM((n_tp, groups, 2 * HEAD, rows), BF16),
            VMEM((rows, n_tp * groups * 2 * HEAD), BF16),
            dma((9,)), dma((n_sp,)), dma((n_sp,)), dma((n_tp,)), dma((n_tp,)),
            dma((n_y, l_chunks)), dma((n_tp, l_chunks)), dma((1 + n_y, l_chunks)), dma((n_tp, l_chunks)),
            dma((n_tiles, groups)), dma((groups, n_tiles)),
            dma((n_tiles, n_sp)), dma((n_sp, n_tiles)), dma((n_tiles, n_sp)), dma((n_sp, n_tiles)),
            dma((n_sp,)), dma((n_sp,)),
            dma((n_y, pieces)), dma((n_tp, pieces)), dma((n_y, shared)), dma((n_tp, shared)),
            dma((n_y, pieces)), dma((n_tp, pieces)), dma, dma,
            dma((n_tiles, groups, per_tile)), dma((n_tp, groups)),
        ],
        compiler_params=pltpu.CompilerParams(
            collective_id=0, has_side_effects=True, vmem_limit_bytes=60 * 1024 * 1024
        ),
    )(
        latent, context, conditioning[None], context_conditioning[None],
        shift_weight, scale_weight, gate_weight, norm_gain[None],
        query_weight, key_weight, value_weight,
        query_gain[None], key_gain[None], context_lift, output_weight.reshape(wo_shape),
    )


def solution(mesh):
    n_sp, n_tp = mesh.shape["sp"], mesh.shape["tp"]
    in_specs = (
        P(("sp", "tp"), None), P("sp", None), P("sp"), P("sp"),
        P("sp", "tp"), P("sp", "tp"), P("sp", "tp"), P(),
        P(None, "tp"), P(None, "tp"), P(None, "tp"), P(), P(), P("tp"), P("tp", None),
    )
    body = functools.partial(shards, n_sp, n_tp)
    return jax.shard_map(body, mesh=mesh, in_specs=in_specs, out_specs=P(("sp", "tp"), None), check_vma=False)
```

```python
import functools
import math

import jax
import jax.numpy as jnp
from jax import lax
from jax.experimental import pallas as pl
from jax.experimental.pallas import tpu as pltpu
from jax.sharding import PartitionSpec as P

HEAD = 64
GRID = 64
EPSILON = 1e-06
ROTARY_BASE = 10000.0
F32 = jnp.float32
BF16 = jnp.bfloat16
VMEM = pltpu.VMEM
TILE = 256
ONES = 16
NT_DIMS = (((1,), (1,)), ((), ()))


def dot(a, b):
    return jnp.dot(a, b, preferred_element_type=F32)


def dot_nt(a, b):
    return lax.dot_general(a, b, NT_DIMS, preferred_element_type=F32)


def remote(src, dst, send, recv, sp, tp):
    return pltpu.make_async_remote_copy(
        src_ref=src,
        dst_ref=dst,
        send_sem=send,
        recv_sem=recv,
        device_id=(sp, tp),
        device_id_type=pl.DeviceIdType.MESH,
    )


def loop(low, high, body):
    def step(i, _):
        body(i)
        return 0

    lax.fori_loop(low, high, step, 0)


def few(low, high, body):
    if high - low > 16:
        loop(low, high, body)
    else:
        for i in range(low, high):
            body(i)


def fused_kernel(
    n_sp, n_tp, groups, n_x, n_z, plain, l_chunks,
    latent_h, context_h, cond, ctx_cond, shift_h, scale_h, gate_h, gain,
    wq_h, wk_h, wv_h, q_gain, k_gain, lift, wo_h,
    out,
    lat, ctxp, shift_w, scale_w, gate_w, wq, wk, wv, w_t, wo_all,
    part, total, recv1, recv2, mods, rows8, hid, cos_t, sin_t,
    qst, kst, vst, cst, qin, kin, vin, cin, kcx, vcx, qbd,
    sa, sb, m_ref, acc, ost, att_t, att,
    loads, s1, r1, s2, r2, sy, ry, sfw, rp,
    sq, rq, sk, rk, sv, rv, sc, rc,
    swy, rwy, swx, rwx, swp, rwp, swo, rwo, s_out, r_out,
):
    me = lax.axis_index("sp")
    t = lax.axis_index("tp")
    n_y = n_tp // 2
    y, c = t // 2, t % 2
    partner = y * 2 + 1 - c
    halves = n_sp // groups
    half, g = me // groups, me % groups
    rows, model = lat.shape[1], lat.shape[2]
    per_tile = TILE // rows
    n_tiles = rows * n_tp // TILE
    y_per = per_tile // 2
    own_block = t // per_tile
    c_rows = context_h.shape[0]
    width = total.shape[1]

    def block(k):
        return lax.rem(own_block + k, n_tiles)

    barrier = pltpu.get_barrier_semaphore()

    def greet(sp, tp):
        pl.semaphore_signal(barrier, inc=1, device_id=(sp, tp), device_id_type=pl.DeviceIdType.MESH)

    def greet_half(i):
        to = lax.rem(t + 1 + i // groups, n_tp)
        greet(half * groups + lax.rem(g + i, groups), to)

    few(1, n_sp, lambda j: greet(lax.rem(me + j, n_sp), t))
    few(0, groups * (n_tp - 1), greet_half)
    fetch = [
        pltpu.make_async_copy(src, dst, loads.at[i])
        for i, (src, dst) in enumerate(
            (
                (latent_h, lat.at[t]), (shift_h, shift_w), (scale_h, scale_w), (gate_h, gate_w),
                (wq_h, wq), (wk_h, wk), (wv_h, wv),
                (context_h, ctxp.at[pl.ds(0, c_rows)]), (wo_h, wo_all.at[t]),
            )
        )
    ]
    for copy in fetch:
        copy.start()
    pl.semaphore_wait(barrier, n_sp - 1 + groups * (n_tp - 1))

    piece = rows // l_chunks
    fetch[0].wait()

    def y_copy(k, ch):
        other = lax.rem(y + k, n_y)
        part_of = lat.at[t, pl.ds(ch * piece, piece)]
        return remote(part_of, part_of, sy.at[k, ch], ry.at[t, ch], me, other * 2 + c)

    def y_start(ch):
        loop(1, n_y, lambda k: y_copy(k, ch).start())

    early = (l_chunks + 1) * 2 // 5
    early = max(early, 1)
    for ch in range(early):
        y_start(ch)
    own_partner = remote(lat.at[t], lat.at[t], sfw.at[0, 0], rp.at[t, 0], me, partner)
    own_partner.start()

    shape8 = (8, cond.shape[1])
    row8 = lax.broadcasted_iota(jnp.int32, shape8, 0)
    a = jnp.broadcast_to(cond[...] / (1.0 + jnp.exp(-cond[...])), shape8)
    b = jnp.broadcast_to(ctx_cond[...] / (1.0 + jnp.exp(-ctx_cond[...])), shape8)
    first = jnp.where(row8 == 0, a, jnp.where(row8 == 1, b, 0.0)).astype(BF16)
    second = jnp.where(row8 == 2, a, jnp.where(row8 == 3, b, 0.0)).astype(BF16)
    third = jnp.where(row8 == 4, a, 0.0).astype(BF16)
    for copy in fetch[1:4]:
        copy.wait()
    mine = dot(first, shift_w[...]) + dot(second, scale_w[...]) + dot(third, gate_w[...])
    part[...] = mine
    recv1[me] = mine

    def mod_copy(j):
        return remote(part, recv1.at[me], s1.at[j], r1.at[me], lax.rem(me + j, n_sp), t)

    loop(1, n_sp, lambda j: mod_copy(j).start())

    for copy in fetch[4:7]:
        copy.wait()

    def turn_weights(i):
        span = pl.ds(pl.multiple_of(i * TILE, TILE), TILE)
        q_rows, k_rows, v_rows = (jnp.transpose(w[span, :]) for w in (wq, wk, wv))
        for j in range(groups):
            w_t[j, 0 : 2 * HEAD, span] = q_rows[2 * HEAD * j : 2 * HEAD * (j + 1), :]
            w_t[j, 2 * HEAD : 3 * HEAD, span] = k_rows[HEAD * j : HEAD * (j + 1), :]
            w_t[j, 3 * HEAD : 4 * HEAD, span] = v_rows[HEAD * j : HEAD * (j + 1), :]

    n_turns = model // TILE
    loop(0, n_turns // 2, turn_weights)

    def mod_wait(j):
        src = lax.rem(me + j, n_sp)
        pltpu.make_async_copy(recv1.at[src], recv1.at[src], r1.at[src]).wait()

    loop(1, n_sp, mod_wait)
    summed = lax.fori_loop(1, n_sp, lambda j, s: s + recv1[j], recv1[0])
    total[...] = summed
    recv2[t] = summed

    def tot_copy(j):
        return remote(total, recv2.at[t], s2.at[j], r2.at[t], me, lax.rem(t + j, n_tp))

    loop(1, n_tp, lambda j: tot_copy(j).start())
    for ch in range(early, l_chunks):
        y_start(ch)

    loop(n_turns // 2, n_turns, turn_weights)

    channel = lax.broadcasted_iota(jnp.int32, (HEAD, TILE), 0)
    lane = lax.broadcasted_iota(jnp.int32, (HEAD, TILE), 1)
    quarter = HEAD // 4
    power = ((channel // 2) % quarter).astype(F32)
    frequency = jnp.exp(power * (-math.log(ROTARY_BASE) / quarter))
    even = channel % 2 == 0

    def tables(i):
        position = (me * n_tiles + i) * TILE + lane
        place = jnp.where(channel < HEAD // 2, position // GRID, position % GRID)
        angle = place.astype(F32) * frequency
        cos_t[i] = jnp.cos(angle)
        sine = jnp.sin(angle)
        sin_t[i] = jnp.where(even, -sine, sine)

    loop(0, n_tiles, tables)

    def blank(i):
        qbd[i] = jnp.zeros(qbd.shape[1:], BF16)

    loop(0, qbd.shape[0], blank)

    def ones(ref, i):
        ref[i, HEAD:, :] = jnp.ones((ONES, TILE), BF16)

    loop(0, vin.shape[0], lambda i: ones(vin, i))
    loop(0, vcx.shape[0], lambda i: ones(vcx, i))

    def tot_wait(j):
        src = lax.rem(t + j, n_tp)
        pltpu.make_async_copy(recv2.at[src], recv2.at[src], r2.at[src]).wait()

    loop(1, n_tp, tot_wait)
    for j in range(n_tp):
        mods[:, j * width : (j + 1) * width] = recv2[j]
    for i, (shift_row, scale_row) in enumerate(((0, 2), (1, 3))):
        factor = gain[...] * (1.0 + mods[scale_row : scale_row + 1, :])
        rows8[2 * i] = jnp.broadcast_to(factor, (8, model))
        rows8[2 * i + 1] = jnp.broadcast_to(mods[shift_row : shift_row + 1, :], (8, model))

    step_rows = 32

    def hidden_of(x, which):
        x = x.astype(F32)
        inv = lax.rsqrt(jnp.mean(x * x, axis=-1, keepdims=True) + EPSILON)
        x = (x * inv).reshape(x.shape[0] // 8, 8, model)
        return (x * rows8[2 * which][None] + rows8[2 * which + 1][None]).reshape(-1, model)

    def column(row):
        turned = jnp.transpose(jnp.broadcast_to(row[...], (128, HEAD)))
        return jnp.concatenate([turned] * (TILE // 128), axis=1)

    q_gains, k_gains = column(q_gain), column(k_gain)

    def norm(v, gains):
        mean = jnp.mean(v * v, axis=0, keepdims=True)
        return v * lax.rsqrt(mean + EPSILON) * gains

    def turn(v, cos_v, sin_v):
        v3 = v.reshape(HEAD // 8, 8, TILE)
        pairs = lax.broadcasted_iota(jnp.int32, v3.shape, 1) % 2 == 0
        swapped = jnp.where(pairs, pltpu.roll(v3, 7, 1), pltpu.roll(v3, 1, 1)).reshape(HEAD, TILE)
        return v * cos_v + swapped * sin_v

    def q_copy(bk, j, to):
        return remote(qst.at[bk, j], qin.at[g, bk], sq.at[bk, to], rq.at[g, bk], half * groups + j, t)

    def kv_copies(bk, n):
        j = lax.rem(g + n, groups)
        to = lax.rem(half + n // groups, halves) * groups + j
        slot = me * n_tiles + bk
        return (
            remote(kst.at[bk, j], kin.at[slot], sk.at[bk, n], rk.at[me, bk], to, t),
            remote(
                vst.at[bk, j], vin.at[slot, pl.ds(0, HEAD)], sv.at[bk, n], rv.at[me, bk], to, t
            ),
        )

    def hide(owner):
        base = lax.rem(owner, per_tile) * rows

        def one(i):
            x = lat[owner, pl.ds(i * step_rows, step_rows), :]
            start = pl.multiple_of(base + i * step_rows, step_rows)
            hid[pl.ds(start, step_rows), :] = hidden_of(x, 0).astype(BF16)

        loop(0, rows // step_rows, one)

    border = (half == 0) == (g >= groups // 2) if halves == 2 else g >= 0

    def project(bk):
        cos_v, sin_v = cos_t[bk], sin_t[bk]
        order = [lax.rem(g + n, groups) for n in list(range(1, groups)) + [0]]
        ahead = dot_nt(w_t[order[0]], hid[...])
        for place, j in enumerate(order):
            z = ahead
            if place + 1 < groups:
                ahead = dot_nt(w_t[order[place + 1]], hid[...])
            for i in range(2):
                q = turn(norm(z[HEAD * i : HEAD * (i + 1)], q_gains), cos_v, sin_v)
                qst[bk, j, i] = (q.astype(BF16).astype(F32) * HEAD ** (-0.5)).astype(BF16)
            k = turn(norm(z[2 * HEAD : 3 * HEAD], k_gains), cos_v, sin_v)
            k = jnp.concatenate([k[:, :128], k[:, 128:]], axis=0)
            kst[bk, j] = jnp.transpose(k).astype(BF16)
            vst[bk, j] = z[3 * HEAD :].astype(BF16)
            n = (place + 1) % groups
            if n:
                q_copy(bk, j, n).start()
                for copy in kv_copies(bk, n):
                    copy.start()

            @pl.when(border)
            def _(n=n):
                for d in range(1, halves):
                    for copy in kv_copies(bk, d * groups + n):
                        copy.start()

        qin[g, bk] = qst[bk, g]
        kin[me * n_tiles + bk] = kst[bk, g]
        vin[me * n_tiles + bk, 0:HEAD, :] = vst[bk, g]

    def cross(bk):
        def one(n):
            for copy in kv_copies(bk, n):
                copy.start()

        loop(groups, n_sp, one)

    def y_near(other):
        return other * 2 + c, other * 2 + 1 - c

    def forward(other, ch):
        near, _ = y_near(other)
        part_of = lat.at[near, pl.ds(ch * piece, piece)]
        return remote(part_of, part_of, sfw.at[1 + other, ch], rp.at[near, ch], me, partner)

    def take(other):
        near, far = y_near(other)
        for ch in range(l_chunks):
            part_of = lat.at[near, pl.ds(ch * piece, piece)]
            pltpu.make_async_copy(part_of, part_of, ry.at[near, ch]).wait()
            forward(other, ch).start()
        hide(near)
        for ch in range(l_chunks):
            part_of = lat.at[far, pl.ds(ch * piece, piece)]
            pltpu.make_async_copy(part_of, part_of, rp.at[far, ch]).wait()
        hide(far)

    hide(t)
    pltpu.make_async_copy(lat.at[partner], lat.at[partner], rp.at[partner, 0]).wait()
    hide(partner)
    if y_per > 1:
        loop(1, y_per, lambda o: take(own_block * y_per + lax.rem(y % y_per + o, y_per)))
    project(block(0))
    fetch[7].wait()
    c_lane = lax.broadcasted_iota(jnp.int32, (HEAD, 128), 1)

    def hide_context(i):
        span = pl.ds(pl.multiple_of(i * step_rows, step_rows), step_rows)
        row = i * step_rows + lax.broadcasted_iota(jnp.int32, (step_rows, model), 0)
        keep = row < c_rows
        h = hidden_of(jnp.where(keep, ctxp[span, :].astype(F32), 0.0), 1)
        hid[span, :] = jnp.where(keep, h, 0.0).astype(BF16)

    loop(0, 128 // step_rows, hide_context)
    for j in range(groups):
        z = dot_nt(w_t[j, 2 * HEAD :], hid[0:128, :])
        k = norm(z[:HEAD], k_gains[:, :128])
        cst[j] = jnp.where(c_lane < HEAD, k, pltpu.roll(z[HEAD:], HEAD, 1)).astype(BF16)

    def c_copy(n):
        to = lax.rem(half + n // groups, halves) * groups + lax.rem(g + n, groups)
        return remote(cst.at[lax.rem(g + n, groups)], cin.at[me], sc.at[n], rc.at[me], to, t)

    loop(1, n_sp, lambda n: c_copy(n).start())
    cin[me] = cst[g]

    fetch[8].wait()
    shared = n_x + n_z
    side_x, side_z = me % 2, g // (groups // 2 if groups > 1 else 1) % 2
    across_x = me + 1 - 2 * side_x
    across_z = half * groups + lax.rem(g + groups // 2, groups)

    def w_ref(owner, at):
        return wo_all.at[owner, at]

    def w_at(ch, mine=True):
        if ch < n_x:
            return (side_x if mine else 1 - side_x) * n_x + ch
        if ch < shared:
            return 2 * n_x + (side_z if mine else 1 - side_z) * n_z + ch - n_x
        return shared + ch

    def w_y(k, ch):
        other = lax.rem(y + k, n_y)
        ref = w_ref(t, w_at(ch))
        return remote(ref, ref, swy.at[k, ch], rwy.at[t, ch], me, other * 2 + c)

    def w_x(other, ch):
        near, _ = y_near(other)
        ref = w_ref(near, w_at(ch))
        return remote(ref, ref, swx.at[other, ch], rwx.at[near, ch], across_x if ch < n_x else across_z, t)

    def w_p(other, ch, mine=True):
        near, _ = y_near(other)
        at = w_at(ch, mine)
        ref = w_ref(near, at)
        return remote(ref, ref, swp.at[other, at], rwp.at[near, at], me, partner)

    w_own = remote(wo_all.at[t], wo_all.at[t], swo, rwo, me, partner)

    def over_y(body):
        loop(1, n_y, lambda k: body(lax.rem(y + n_y - k, n_y)))

    def forward_y(ch, to_x=True):
        def one(other):
            near, _ = y_near(other)
            ref = w_ref(near, w_at(ch))
            pltpu.make_async_copy(ref, ref, rwy.at[near, ch]).wait()
            if to_x:
                w_x(other, ch).start()
            w_p(other, ch).start()

        over_y(one)

    def forward_x(ch):
        def one(other):
            near, _ = y_near(other)
            ref = w_ref(near, w_at(ch, False))
            pltpu.make_async_copy(ref, ref, rwx.at[near, ch]).wait()
            w_p(other, ch, False).start()

        over_y(one)

    def forward_plain(ch):
        forward_y(shared + ch, False)

    for ch in range(shared + plain):
        loop(1, n_y, lambda k, ch=ch: w_y(k, ch).start())

    for k in range(1, n_tiles):
        loop(0, y_per, lambda o, k=k: take(block(k) * y_per + o))
        project(block(k))
    w_own.start()

    @pl.when(jnp.logical_not(border))
    def _():
        for k in range(n_tiles):
            cross(block(k))

    def wait_kv(d, k, low, high, first):
        bk = block(k)

        def one(i):
            s = lax.rem(half + d, halves) * groups + lax.rem(first + i, groups)
            slot = s * n_tiles + bk
            pltpu.make_async_copy(kin.at[slot], kin.at[slot], rk.at[s, bk]).wait()
            ref = vin.at[slot, pl.ds(0, HEAD)]
            pltpu.make_async_copy(ref, ref, rv.at[s, bk]).wait()

        loop(low, high, one)

    def wait_queries(k):
        bk = block(k)

        def one(i):
            j = lax.rem(g + i, groups)
            pltpu.make_async_copy(qin.at[j, bk], qin.at[j, bk], rq.at[j, bk]).wait()

        loop(1, groups, one)

        def spread(j):
            for i in range(2):
                q = qin[j, bk, i]
                slot = (j * n_tiles + bk) * 2 + i
                qbd[slot, 0:HEAD, 0:TILE] = q
                qbd[slot, HEAD:, TILE:] = q

        loop(0, groups, spread)

    def wait_own(k):
        wait_queries(k)
        wait_kv(0, k, 1, groups, g)

    def wait_cross(d, k):
        wait_kv(d, k, 0, groups, 0)

    def wait_context():
        def one(j):
            s = lax.rem(me + j, n_sp)
            pltpu.make_async_copy(cin.at[s], cin.at[s], rc.at[s]).wait()

        loop(1, n_sp, one)
        per = 128 // c_rows
        for u in range(kcx.shape[0]):
            keys, values = [], []
            for m in (2 * u, 2 * u + 1):
                k = v = jnp.zeros((HEAD, 128), F32)
                for i in range(per):
                    at = i * c_rows
                    both = cin[m * per + i].astype(F32)
                    keep = (c_lane >= at) & (c_lane < at + c_rows)
                    k = jnp.where(keep, pltpu.roll(both, at, 1) if at else both, k)
                    back = (at - HEAD) % 128
                    v = jnp.where(keep, pltpu.roll(both, back, 1) if back else both, v)
                keys.append(k)
                values.append(v)
            kcx[u] = jnp.transpose(jnp.concatenate(keys, axis=0)).astype(BF16)
            vcx[u, 0:HEAD, :] = jnp.concatenate(values, axis=1).astype(BF16)

    def slabs(d, k, first=0, count=groups):
        base = lax.rem(half + d, halves) * groups
        slots = [(base + first + i) * n_tiles + block(k) for i in range(count)]
        return [(kin, vin, slot, False) for slot in slots]

    context = [(kcx, vcx, u, True) for u in range(kcx.shape[0])]

    def out_copy(bk, j, p):
        return remote(
            ost.at[bk, j, p], att_t.at[t, g], s_out.at[bk, j, p], r_out.at[t, g],
            half * groups + j, bk * per_tile + p,
        )

    def sweep(k, blocks, start, final):
        bk = block(k)

        def slot_of(j, i):
            return (lax.rem(g + 1 + j, groups) * n_tiles + bk) * 2 + i

        def scores(j, i, dst):
            q = qbd[slot_of(j, i)]
            top = None
            for place, (keys, _, slot, lifted) in enumerate(blocks):
                s = dot(keys[slot], q)
                if lifted:
                    s = s + lift[g * 2 + i]
                dst[place] = s
                peak = jnp.max(s.reshape(s.shape[0] // 8, 8, s.shape[1]), axis=0)
                top = peak if top is None else jnp.maximum(top, peak)
            return top

        def soft(j, i, src, top):
            slot = slot_of(j, i)
            top = jnp.max(top, axis=0, keepdims=True)
            top = jnp.maximum(top[:, :TILE], top[:, TILE:])
            if not start:
                old = m_ref[slot, 0:1, :]
                top = jnp.maximum(old, top)
            wide = jnp.concatenate([top, top], axis=1)
            weights = []
            for place in range(len(blocks)):
                w = jnp.exp(src[place] - wide).astype(BF16)
                weights += [w[:, :TILE], w[:, TILE:]]
            values = jnp.concatenate([v[at] for _, v, at, _ in blocks], axis=1)
            o = dot(values, jnp.concatenate(weights, axis=0))
            if not start:
                o = acc[slot] * jnp.exp(old - top) + o
            if not final:
                acc[slot] = o
                m_ref[slot] = jnp.broadcast_to(top, (8, TILE))
                return
            o = (o[:HEAD] / o[HEAD : HEAD + 1]).astype(BF16)
            to = lax.rem(g + 1 + j, groups)
            for p in range(per_tile):
                ost[bk, to, p, i * HEAD : (i + 1) * HEAD, :] = o[:, p * rows : (p + 1) * rows]

        def pair(j, top):
            later = scores(j, 1, sb)
            soft(j, 0, sa, top)
            return later

        def body(j, top):
            later = pair(j, top)
            top = scores(j + 1, 0, sa)
            soft(j, 1, sb, later)
            if final:
                for p in range(per_tile):
                    out_copy(bk, lax.rem(g + 1 + j, groups), p).start()
            return top

        top = scores(0, 0, sa)
        top = lax.fori_loop(0, groups - 1, body, top)
        later = pair(groups - 1, top)
        soft(groups - 1, 1, sb, later)
        if final:
            for p in range(per_tile):
                if k:
                    out_copy(bk, g, p).start()
                else:

                    @pl.when(p != t % per_tile)
                    def _(p=p):
                        out_copy(bk, g, p).start()

            if k == 0:
                att_t[t, g] = ost[bk, g, t % per_tile]

    if n_tiles == 2 and halves == 2 and groups == 4 and shared == 6:
        near_g = jnp.where(half == 0, 0, groups // 2)
        far_g = groups // 2 - near_g
        near, close = slabs(1, 0, near_g, 2), slabs(1, 1, near_g, 2)
        far0, far1 = slabs(1, 0, far_g, 2), slabs(1, 1, far_g, 2)
        wait_own(0)
        forward_y(0)
        sweep(0, slabs(0, 0), True, False)
        forward_y(1)
        wait_kv(1, 0, 0, 2, near_g)
        wait_context()
        forward_y(2)
        sweep(0, near + context, False, False)
        wait_queries(1)
        forward_y(3)
        sweep(1, slabs(0, 0) + context + near, True, False)
        forward_y(4)
        forward_y(5)
        wait_kv(0, 1, 1, groups, g)
        forward_x(0)
        forward_x(1)
        sweep(0, slabs(0, 1), False, False)
        wait_kv(1, 1, 0, 2, near_g)
        wait_kv(1, 0, 0, 2, far_g)
        wait_kv(1, 1, 0, 2, far_g)
        far = close + far0 + far1
        forward_plain(0)
        sweep(1, slabs(0, 1) + far, False, True)
        forward_plain(1)
        forward_plain(2)
        forward_x(2)
        forward_x(3)
        sweep(0, far, False, True)
        forward_plain(3)
        forward_x(4)
        forward_x(5)
    else:
        for k in range(n_tiles):
            wait_own(k)
        wait_context()
        for k in range(n_tiles):
            own = [slab for i in range(n_tiles) for slab in slabs(0, i)]
            sweep(k, own + context, True, halves == 1)

        def further(d, final):
            for i in range(n_tiles):
                wait_cross(d, i)
            for k in range(n_tiles):
                sweep(k, [slab for i in range(n_tiles) for slab in slabs(d, i)], False, final)

        if halves > 1:
            loop(1, halves - 1, lambda d: further(d, False))
            further(halves - 1, True)
        for ch in range(shared):
            forward_y(ch)
        for ch in range(plain):
            forward_plain(ch)
        for ch in range(shared):
            forward_x(ch)

    ref = wo_all.at[partner]
    pltpu.make_async_copy(ref, ref, rwo).wait()

    def w_far(k):
        _, far = y_near(lax.rem(y + n_y - k, n_y))
        for at in range(2 * shared + plain):
            ref = w_ref(far, at)
            pltpu.make_async_copy(ref, ref, rwp.at[far, at]).wait()

    loop(1, n_y, w_far)

    def out_wait(i):
        at = lax.rem(t * groups + g + i, n_tp * groups)
        ref = att_t.at[at // groups, at % groups]
        pltpu.make_async_copy(ref, ref, r_out.at[at // groups, at % groups]).wait()

    loop(1, n_tp * groups, out_wait)
    for i in range(n_tp):
        for j in range(groups):
            at = (i * groups + j) * 2 * HEAD
            att[:, at : at + 2 * HEAD] = jnp.transpose(att_t[i, j])
    n_out = 4
    wide = model // n_out
    for n in range(n_out):
        span = slice(n * wide, (n + 1) * wide)
        weight = wo_all[:, :, :, span].reshape(-1, wide)
        projection = dot(att[...], weight)
        out[:, span] = (lat[t, :, span].astype(F32) + mods[4:5, span] * projection).astype(BF16)

    own_partner.wait_send()
    w_own.wait_send()

    def drain_y(k):
        other = lax.rem(y + k, n_y)
        for ch in range(l_chunks):
            y_copy(k, ch).wait_send()
            forward(other, ch).wait_send()
        for ch in range(shared + plain):
            w_y(k, ch).wait_send()
            w_p(other, ch).wait_send()
        for ch in range(shared):
            w_x(other, ch).wait_send()
            w_p(other, ch, False).wait_send()

    loop(1, n_y, drain_y)
    loop(1, n_sp, lambda j: mod_copy(j).wait_send())
    loop(1, n_tp, lambda j: tot_copy(j).wait_send())

    def drain_sp(n):
        c_copy(n).wait_send()
        for bk in range(n_tiles):
            for copy in kv_copies(bk, n):
                copy.wait_send()

    loop(1, n_sp, drain_sp)
    for bk in range(n_tiles):
        loop(1, groups, lambda n, bk=bk: q_copy(bk, lax.rem(g + n, groups), n).wait_send())

        def drain_out(j, bk=bk):
            for p in range(per_tile):

                @pl.when(jnp.logical_or(j != g, bk * per_tile + p != t))
                def _(p=p):
                    out_copy(bk, j, p).wait_send()

        loop(0, groups, drain_out)


def shards(
    n_sp, n_tp,
    latent, context, conditioning, context_conditioning, shift_weight, scale_weight, gate_weight,
    norm_gain, query_weight, key_weight, value_weight, query_gain, key_gain, context_lift, output_weight,
):
    k_heads = key_weight.shape[1] // HEAD
    q_heads = query_weight.shape[1] // HEAD
    rows, model = latent.shape
    c_rows = context.shape[0]
    o_rows = output_weight.shape[0]
    part_width = shift_weight.shape[1]
    assert q_heads == 2 * k_heads and n_sp % k_heads == 0 and n_sp % 2 == 0
    assert TILE % rows == 0 and rows * n_tp % TILE == 0 and 2 * c_rows <= 128
    groups = k_heads
    per_tile = TILE // rows
    n_tiles = rows * n_tp // TILE
    n_context = n_sp * c_rows // TILE
    n_x, n_z, plain = (4, 2, 4) if o_rows >= 256 and groups == 4 else (1, 0, 0)
    shared = n_x + n_z
    pieces = 2 * shared + plain
    l_chunks = 8 if rows >= 128 else 1
    most = groups * n_tiles * 2 + n_context
    n_q = groups * n_tiles * 2
    n_y = n_tp // 2
    vmem = pl.BlockSpec(memory_space=VMEM)
    dma = pltpu.SemaphoreType.DMA
    hbm = pl.BlockSpec(memory_space=pltpu.HBM)
    smem = pl.BlockSpec(memory_space=pltpu.SMEM)
    wo_shape = (pieces, o_rows // pieces, model)
    return pl.pallas_call(
        functools.partial(fused_kernel, n_sp, n_tp, groups, n_x, n_z, plain, l_chunks),
        name="fused",
        out_shape=jax.ShapeDtypeStruct((rows, model), BF16),
        in_specs=[
            hbm, hbm, vmem, vmem, hbm, hbm, hbm, vmem, hbm, hbm, hbm, vmem, vmem, smem, hbm,
        ],
        out_specs=vmem,
        scratch_shapes=[
            VMEM((n_tp, rows, model), BF16), VMEM((128, model), BF16),
            VMEM(shift_weight.shape, BF16), VMEM(scale_weight.shape, BF16), VMEM(gate_weight.shape, BF16),
            VMEM(query_weight.shape, BF16), VMEM(key_weight.shape, BF16), VMEM(value_weight.shape, BF16),
            VMEM((groups, 4 * HEAD, model), BF16),
            VMEM((n_tp,) + wo_shape, BF16),
            VMEM((8, part_width), F32), VMEM((8, part_width), F32),
            VMEM((n_sp, 8, part_width), F32), VMEM((n_tp, 8, part_width), F32),
            VMEM((8, model), F32), VMEM((4, 8, model), F32),
            VMEM((TILE, model), BF16),
            VMEM((n_tiles, HEAD, TILE), F32), VMEM((n_tiles, HEAD, TILE), F32),
            VMEM((n_tiles, groups, 2, HEAD, TILE), BF16),
            VMEM((n_tiles, groups, 128, 128), BF16),
            VMEM((n_tiles, groups, HEAD, TILE), BF16),
            VMEM((groups, HEAD, 128), BF16),
            VMEM((groups, n_tiles, 2, HEAD, TILE), BF16),
            VMEM((n_sp * n_tiles, 128, 128), BF16),
            VMEM((n_sp * n_tiles, HEAD + ONES, TILE), BF16),
            VMEM((n_sp, HEAD, 128), BF16),
            VMEM((n_context, 128, 128), BF16),
            VMEM((n_context, HEAD + ONES, TILE), BF16),
            VMEM((n_q, 128, 2 * TILE), BF16),
            VMEM((most, 128, 2 * TILE), F32), VMEM((most, 128, 2 * TILE), F32),
            VMEM((n_q, 8, TILE), F32), VMEM((n_q, HEAD + ONES, TILE), F32),
            VMEM((n_tiles, groups, per_tile, 2 * HEAD, rows), BF16),
            VMEM((n_tp, groups, 2 * HEAD, rows), BF16),
            VMEM((rows, n_tp * groups * 2 * HEAD), BF16),
            dma((9,)), dma((n_sp,)), dma((n_sp,)), dma((n_tp,)), dma((n_tp,)),
            dma((n_y, l_chunks)), dma((n_tp, l_chunks)), dma((1 + n_y, l_chunks)), dma((n_tp, l_chunks)),
            dma((n_tiles, groups)), dma((groups, n_tiles)),
            dma((n_tiles, n_sp)), dma((n_sp, n_tiles)), dma((n_tiles, n_sp)), dma((n_sp, n_tiles)),
            dma((n_sp,)), dma((n_sp,)),
            dma((n_y, pieces)), dma((n_tp, pieces)), dma((n_y, shared)), dma((n_tp, shared)),
            dma((n_y, pieces)), dma((n_tp, pieces)), dma, dma,
            dma((n_tiles, groups, per_tile)), dma((n_tp, groups)),
        ],
        compiler_params=pltpu.CompilerParams(
            collective_id=0, has_side_effects=True, vmem_limit_bytes=60 * 1024 * 1024
        ),
    )(
        latent, context, conditioning[None], context_conditioning[None],
        shift_weight, scale_weight, gate_weight, norm_gain[None],
        query_weight, key_weight, value_weight,
        query_gain[None], key_gain[None], context_lift, output_weight.reshape(wo_shape),
    )


def solution(mesh):
    n_sp, n_tp = mesh.shape["sp"], mesh.shape["tp"]
    in_specs = (
        P(("sp", "tp"), None), P("sp", None), P("sp"), P("sp"),
        P("sp", "tp"), P("sp", "tp"), P("sp", "tp"), P(),
        P(None, "tp"), P(None, "tp"), P(None, "tp"), P(), P(), P("tp"), P("tp", None),
    )
    body = functools.partial(shards, n_sp, n_tp)
    return jax.shard_map(body, mesh=mesh, in_specs=in_specs, out_specs=P(("sp", "tp"), None), check_vma=False)
```
